32 devices in a mesh: grp: 2 (over x), sp: 4 (over z), tp: 4 (over y, core).
Axes of the slice: x: 2, y: 2, z: 4, core: 2. Of those that a mesh axis runs over, the one named last changes fastest.
Arguments:
- grid_tokens: bfloat16 [64, 64, 1024], P(('grp', 'sp'), 'tp'), parts along dimension 0, may hold values from -6 to 6
- norm_gain: float32 [2, 1024], replicated, may hold values from 0.1 to 1.9
- w_query: bfloat16 [2, 1024, 512], replicated, may hold values from -0.84375 to 0.84375
- w_key: bfloat16 [2, 1024, 512], replicated, may hold values from -1.1390625 to 1.1390625
- w_value: bfloat16 [2, 1024, 512], replicated, may hold values from -0.1875 to 0.1875
- offset_bias: float32 [2, 4, 15, 31], replicated, may hold values from -5 to 5
- w_out: bfloat16 [2, 512, 1024], replicated, may hold values from -1 to 1
Outputs:
- grid_out: bfloat16 [64, 64, 1024], P(('grp', 'sp'), 'tp'), parts along dimension 0
The draws below stay inside these ranges and needn't reach their ends.
There are 2 independent parts, one for each index of `grp`. The reference program is written for one: setup_inputs(seed, part) draws one part's arguments, and reference() takes and returns one part's arrays. A program takes and returns all parts, laid end to end along the dimension named above; an argument that names none is the same for every part. Nothing has to cross between parts.
All inputs are finite; a program needn't handle non-finite values.
Results may differ from the reference program's by a relative error of at most 0.014.
Values may be sent and summed in bfloat16 or wider, within the bound.
A program may use at most 64 MiB of HBM per device.

```python
import jax
import jax.numpy as jnp
from jax import lax

D = 1024
HEADS = 4
HEAD_DIM = 128
WIN_ROWS = 8
WIN_COLS = 16
LAYERS = 2
GRID_ROWS = 32
GRID_COLS = 64


def query_key_pair(key):
    base = jax.random.fold_in(key, 7)
    first_key, second_key = jax.random.split(base, 2)
    shape = (LAYERS, D, HEADS * HEAD_DIM)
    first = jnp.clip(jax.random.normal(first_key, shape, jnp.float32), -6.0, 6.0)
    second = jnp.clip(jax.random.normal(second_key, shape, jnp.float32), -6.0, 6.0)
    query_part = first
    key_part = second
    factor = D ** (-0.5)
    return (query_part * factor, key_part * factor)


def draw_w_query(key, part):
    return query_key_pair(key)[0].astype(jnp.bfloat16)


def draw_w_key(key, part):
    return query_key_pair(key)[1].astype(jnp.bfloat16)


def shard_levels(key, shape, cuts, smallest, high):
    def one(dim, parts):
        steps = jax.random.uniform(jax.random.fold_in(jax.random.fold_in(key, 6), dim), (parts,), jnp.float32, smallest / len(cuts), high / len(cuts))
        return jnp.repeat(jnp.exp(steps), shape[dim] // parts).reshape((-1,) + (1,) * (len(shape) - dim - 1))

    factor_of = one(*cuts[0])
    for cut in cuts[1:]:
        factor_of = factor_of * one(*cut)
    return factor_of


def scatter_about(key, extent, spread, reach, cuts=(), kind=jnp.bfloat16):
    drawn = spread * jax.random.normal(key, extent, jnp.float32)
    if cuts:
        drawn = drawn * shard_levels(key, extent, cuts, -0.22, 0.18)
    return jnp.clip(drawn, -reach, reach).astype(kind)


def setup_inputs(seed: int = 0, part: int = 0) -> dict:
    key_of = jax.random.split(jax.random.key(seed), 8)
    own_keys = jax.random.split(jax.random.fold_in(key_of[7], part), 8)
    grid_tokens = scatter_about(own_keys[0], (GRID_ROWS, GRID_COLS, D), 1.0, 6.0, ((0, 4), (1, 4)))
    norm_gain = jnp.clip(1.0 + 0.18 * jax.random.normal(key_of[1], (LAYERS, D), jnp.float32), 0.1, 1.9)
    w_query = draw_w_query(jax.random.fold_in(key_of[7], 71), part)
    w_key = draw_w_key(jax.random.fold_in(key_of[7], 71), part)
    w_value = scatter_about(key_of[4], (LAYERS, D, HEADS * HEAD_DIM), D ** -0.5, 0.1875)
    offset_bias = scatter_about(key_of[5], (LAYERS, HEADS, 2 * WIN_ROWS - 1, 2 * WIN_COLS - 1), 1.0, 5.0, (), jnp.float32)
    w_out = scatter_about(key_of[6], (LAYERS, HEADS * HEAD_DIM, D), (HEADS * HEAD_DIM // 16) ** -0.5, 1.0)
    return dict(grid_tokens=grid_tokens, norm_gain=norm_gain, w_query=w_query, w_key=w_key, w_value=w_value, offset_bias=offset_bias, w_out=w_out)


NORM_EPSILON = 1e-06

def rms_rows(stream, gain):
    values = stream.astype(jnp.float32)
    factor = lax.rsqrt(lax.optimization_barrier(jnp.mean(values * values, axis=-1, keepdims=True)) + NORM_EPSILON)
    return (values * factor * gain).astype(jnp.bfloat16)

def window_mix(queries, keys_in, values_in, bias_table):
    grid_rows, grid_cols, inner = queries.shape
    head_count = bias_table.shape[0]
    inv_root = 1.0 / HEAD_DIM ** 0.5
    col_ids = jnp.arange(grid_cols, dtype=jnp.int32)
    col_start = jnp.clip(col_ids - WIN_COLS // 2, 0, grid_cols - WIN_COLS)
    key_cols = col_start[:, None] + jnp.arange(WIN_COLS, dtype=jnp.int32)[None, :]
    col_offsets = key_cols - col_ids[:, None] + WIN_COLS - 1
    col_bias = bias_table[:, :, col_offsets]

    def one_row(row_id):
        row_start = jnp.clip(row_id - WIN_ROWS // 2, 0, grid_rows - WIN_ROWS).astype(jnp.int32)
        key_rows = lax.dynamic_slice_in_dim(keys_in, row_start, WIN_ROWS, 0)
        value_rows = lax.dynamic_slice_in_dim(values_in, row_start, WIN_ROWS, 0)
        near_keys = key_rows[:, key_cols].reshape(WIN_ROWS, grid_cols, WIN_COLS, head_count, HEAD_DIM).astype(jnp.float32)
        near_values = value_rows[:, key_cols].reshape(WIN_ROWS, grid_cols, WIN_COLS, head_count, HEAD_DIM).astype(jnp.float32)
        row_query = lax.dynamic_index_in_dim(queries, row_id, 0, keepdims=False)
        row_query = row_query.reshape(grid_cols, head_count, HEAD_DIM).astype(jnp.float32)
        scores = jnp.einsum('chd,jckhd->hcjk', row_query, near_keys) * inv_root
        row_offsets = row_start + jnp.arange(WIN_ROWS, dtype=jnp.int32) - row_id + WIN_ROWS - 1
        offset_terms = jnp.take(col_bias, row_offsets, axis=1)
        scores = scores + jnp.transpose(offset_terms, (0, 2, 1, 3))
        top = lax.optimization_barrier(jnp.max(scores, axis=(2, 3), keepdims=True))
        expo = jnp.exp(scores - top)
        attn_weights = (expo / lax.optimization_barrier(jnp.sum(expo, axis=(2, 3), keepdims=True))).astype(jnp.bfloat16)
        mixture = jnp.einsum('hcjk,jckhd->chd', attn_weights.astype(jnp.float32), near_values)
        return mixture.astype(jnp.bfloat16).reshape(grid_cols, inner)
    return lax.map(one_row, jnp.arange(grid_rows, dtype=jnp.int32))

def reference(grid_tokens, norm_gain, w_query, w_key, w_value, offset_bias, w_out):
    stream = grid_tokens
    for layer_index in range(LAYERS):
        normed = rms_rows(stream, norm_gain[layer_index])
        queries = jnp.dot(normed, w_query[layer_index], preferred_element_type=jnp.float32).astype(jnp.bfloat16)
        keys_all = jnp.dot(normed, w_key[layer_index], preferred_element_type=jnp.float32).astype(jnp.bfloat16)
        values_all = jnp.dot(normed, w_value[layer_index], preferred_element_type=jnp.float32).astype(jnp.bfloat16)
        mixture = window_mix(queries, keys_all, values_all, offset_bias[layer_index])
        branch = jnp.dot(mixture, w_out[layer_index], preferred_element_type=jnp.float32)
        stream = (stream.astype(jnp.float32) + branch).astype(jnp.bfloat16)
    return stream
```

```python
import functools
import math

import jax
import jax.numpy as jnp
from jax import lax
from jax.experimental import pallas as pl
from jax.experimental.pallas import tpu as pltpu
from jax.sharding import PartitionSpec as P

HEAD_DIM = 128
WIN_ROWS = 8
WIN_COLS = 16
NORM_EPSILON = 1e-06
HALF_ROWS = WIN_ROWS // 2
HALF_COLS = WIN_COLS // 2
BELOW = WIN_ROWS - HALF_ROWS - 1
CHUNK_HEADS = 2
MESH = pl.DeviceIdType.MESH
LOG2E = math.log2(math.e)
HIDDEN = -1e30

STEPS = ((1, 0), (-1, 0), (1, 1), (1, -1), (-1, 1), (-1, -1), (0, 1), (0, -1))


def kernel(
    x_hbm, gain_hbm, wq_hbm, wk_hbm, wv_hbm, bias_hbm, wo_hbm, out,
    x, gain, wq, wk, wv, wo, bias, flat, wide, hidden, table, kv, normed, queries, acc,
    local_sem, kv_w_sem, w_sem, send_sem, recv_sem,
    *, sp_count, tp_count,
):
    layers, model_width, inner = wq.shape
    tile_rows, tile_cols, _ = x.shape
    tokens = tile_rows * tile_cols
    heads = inner // HEAD_DIM
    chunks = heads // CHUNK_HEADS
    part = CHUNK_HEADS * HEAD_DIM
    slab_rows = tile_rows + WIN_ROWS
    slab_cols = tile_cols + WIN_COLS
    slab = slab_rows * slab_cols
    own_blocks = tile_cols // HALF_COLS
    row_index = lax.axis_index("sp")
    col_index = lax.axis_index("tp")

    def there(dr, dc):
        r, c = row_index + dr, col_index + dc
        return (r >= 0) & (r < sp_count) & (c >= 0) & (c < tp_count)

    first = [
        pltpu.make_async_copy(x_hbm, x, local_sem.at[0]),
        pltpu.make_async_copy(gain_hbm, gain, local_sem.at[1]),
        pltpu.make_async_copy(bias_hbm, bias, local_sem.at[2]),
    ]
    for copy in first:
        copy.start()
    weight_copies = {}

    def fetch(l, names):
        for name in names:
            if name in "qo":
                src, dst = {"q": (wq_hbm, wq), "o": (wo_hbm, wo)}[name]
                copy = pltpu.make_async_copy(src.at[l], dst.at[l], w_sem.at[l, "qo".index(name)])
                copy.start()
                weight_copies[l, name] = copy
            else:
                src, dst = {"k": (wk_hbm, wk), "v": (wv_hbm, wv)}[name]
                i = "kv".index(name)
                copy = pltpu.make_async_copy(src.at[l], dst.at[l], kv_w_sem.at[l, 0, i])
                copy.start()
                weight_copies[l, 0, i] = copy

    every = ["k", "v"]
    fetch(0, every + ["q"])

    barrier = pltpu.get_barrier_semaphore()
    for dr, dc in STEPS:
        @pl.when(there(dr, dc))
        def _():
            pl.semaphore_signal(
                barrier,
                inc=1,
                device_id={"sp": row_index + dr, "tp": col_index + dc},
                device_id_type=MESH,
            )

    own_rows = slice(HALF_ROWS, HALF_ROWS + tile_rows)
    own_cols = slice(1, 1 + own_blocks)

    def spans(dr, dc):
        if dr == 1:
            rows = slice(tile_rows, tile_rows + HALF_ROWS), slice(0, HALF_ROWS)
        elif dr == -1:
            end = HALF_ROWS + tile_rows
            rows = slice(HALF_ROWS, HALF_ROWS + BELOW), slice(end, end + BELOW)
        else:
            rows = own_rows, own_rows
        if dc == 1:
            cols = slice(own_blocks, own_blocks + 1), slice(0, 1)
        elif dc == -1:
            cols = slice(1, 2), slice(1 + own_blocks, 2 + own_blocks)
        else:
            cols = own_cols, own_cols
        return rows, cols

    def halo_copy(l, g, d):
        dr, dc = STEPS[d]
        (src_rows, dst_rows), (src_cols, dst_cols) = spans(dr, dc)
        return pltpu.make_async_remote_copy(
            src_ref=kv.at[l, g, src_rows, src_cols],
            dst_ref=kv.at[l, g, dst_rows, dst_cols],
            send_sem=send_sem.at[l, g, d],
            recv_sem=recv_sem.at[l, g, d],
            device_id={"sp": row_index + dr, "tp": col_index + dc},
            device_id_type=MESH,
        )

    def fill(rows, cols):
        for l in range(layers):
            for g in range(chunks):
                shape = (rows.stop - rows.start, cols.stop - cols.start) + kv.shape[4:]
                kv[l, g, rows, cols] = jnp.zeros(shape, jnp.bfloat16)

    def zero_missing():
        fill(slice(slab_rows - 1, slab_rows), slice(0, own_blocks + 2))
        for dr, dc in STEPS:
            (_, dst_rows), (_, dst_cols) = spans(dr, dc)

            @pl.when(jnp.logical_not(there(-dr, -dc)))
            def _():
                fill(dst_rows, dst_cols)

    def norm(l, stream):
        factor = lax.rsqrt(jnp.mean(stream * stream, axis=-1, keepdims=True) + NORM_EPSILON)
        normed[...] = (stream * factor * gain[l : l + 1]).astype(jnp.bfloat16)

    def project_kv(l, g):
        cols = slice(g * part, (g + 1) * part)
        for i, w in enumerate((wk, wv)):
            if (l, g, i) in weight_copies:
                weight_copies[l, g, i].wait()
            made = jnp.dot(normed[...], w[l, :, cols], preferred_element_type=jnp.float32)
            made = made.reshape(tile_rows, own_blocks, HALF_COLS, part)
            kv[l, g, own_rows, own_cols, :, i * part : (i + 1) * part] = made.astype(jnp.bfloat16)

    def beside(dc):
        return lax.rem(col_index, 2) == (0 if dc == 1 else 1)

    def relay_copy(l, g, d):
        dr, dc = STEPS[d]
        (_, rows), (src_cols, dst_cols) = spans(dr, dc)
        return pltpu.make_async_remote_copy(
            src_ref=kv.at[l, g, rows, src_cols],
            dst_ref=kv.at[l, g, rows, dst_cols],
            send_sem=send_sem.at[l, g, d],
            recv_sem=recv_sem.at[l, g, d],
            device_id={"sp": row_index, "tp": col_index + dc},
            device_id_type=MESH,
        )

    def direct(dr, dc):
        if dr and dc:
            return there(dr, dc) & jnp.logical_not(beside(dc))
        return there(dr, dc)

    def relayed(dr, dc):
        return there(-dr, 0) & there(0, dc) & beside(dc)

    def send(l, g):
        for d, (dr, dc) in enumerate(STEPS):
            @pl.when(direct(dr, dc))
            def _():
                halo_copy(l, g, d).start()

    def receive_near(l, g):
        for d, (dr, dc) in enumerate(STEPS):
            if dc == 0:
                @pl.when(there(-dr, -dc))
                def _():
                    halo_copy(l, g, d).wait_recv()
        for d, (dr, dc) in enumerate(STEPS):
            if dr and dc:
                @pl.when(relayed(dr, dc))
                def _():
                    relay_copy(l, g, d).start()

    def receive_far(l, g):
        for d, (dr, dc) in enumerate(STEPS):
            if dc:
                @pl.when(there(-dr, -dc))
                def _():
                    halo_copy(l, g, d).wait_recv()

    def project_q(l):
        weight_copies[l, "q"].wait()
        made = jnp.dot(normed[...], wq[l], preferred_element_type=jnp.float32)
        queries[...] = (made * (LOG2E / HEAD_DIM**0.5)).astype(jnp.bfloat16)

    def build_hidden():
        k = lax.broadcasted_iota(jnp.int32, (1, slab), 1)
        key_row = k // slab_cols
        key_col = k - key_row * slab_cols
        row0 = row_index * tile_rows
        col0 = col_index * tile_cols
        c = lax.broadcasted_iota(jnp.int32, (tile_cols, 1), 0)
        col_start = jnp.clip(col0 + c - HALF_COLS, 0, tp_count * tile_cols - WIN_COLS)
        col_start = col_start - (col0 - HALF_COLS)
        col_inside = (key_col >= col_start) & (key_col < col_start + WIN_COLS)
        for r in range(tile_rows):
            start = jnp.clip(row0 + r - HALF_ROWS, 0, sp_count * tile_rows - WIN_ROWS)
            start = start - (row0 - HALF_ROWS)
            row_inside = (key_row >= start) & (key_row < start + WIN_ROWS)
            hidden[r * tile_cols : (r + 1) * tile_cols] = jnp.where(
                col_inside & row_inside, 0.0, HIDDEN
            )

    lead = tile_rows - 1 - BELOW

    def build_flat():
        row_count, col_count = 2 * WIN_ROWS - 1, 2 * WIN_COLS - 1
        flat[...] = jnp.zeros_like(flat)
        for l in range(layers):
            for a in range(row_count):
                place = (lead + a) * slab_cols
                flat[l * heads : (l + 1) * heads, place : place + col_count] = bias[l, a] * LOG2E

    def build_table(l):
        width = flat.shape[1]
        shift = (width - (WIN_COLS - 1 - HALF_COLS)) % width
        for h in range(heads):
            row = l * heads + h
            spread = jnp.broadcast_to(flat[row : row + 1, :], (tile_cols, width))
            wide[...] = pltpu.roll(spread, shift, 1, stride=1, stride_axis=0)
            for r in range(tile_rows):
                first_lane = (tile_rows - 1 - r) * slab_cols
                rows = slice(r * tile_cols, (r + 1) * tile_cols)
                table[l, h, rows] = wide[:, first_lane : first_lane + slab] + hidden[rows]

    def attend(l, g):
        everything = kv[l, g].astype(jnp.float32).reshape(slab, 2 * part).astype(jnp.bfloat16)
        mixed = []
        for i in range(CHUNK_HEADS):
            h = g * CHUNK_HEADS + i
            keys = everything[:, i * HEAD_DIM : (i + 1) * HEAD_DIM]
            values = everything[:, part + i * HEAD_DIM : part + (i + 1) * HEAD_DIM]
            scores = lax.dot_general(
                queries[:, h * HEAD_DIM : (h + 1) * HEAD_DIM], keys,
                (((1,), (1,)), ((), ())), preferred_element_type=jnp.float32,
            ) + table[l, h]
            top = jnp.max(scores, axis=1, keepdims=True)
            expo = jnp.exp2(scores - top)
            total = jnp.sum(expo, axis=1, keepdims=True)
            mix = jnp.dot(expo.astype(jnp.bfloat16), values, preferred_element_type=jnp.float32)
            mixed.append((mix / total).astype(jnp.bfloat16))
        mixture = jnp.concatenate(mixed, axis=1)
        acc[...] += jnp.dot(
            mixture, wo[l, g * part : (g + 1) * part, :], preferred_element_type=jnp.float32
        )

    first[0].wait()
    first[1].wait()
    acc[...] = x[...].reshape(tokens, model_width).astype(jnp.float32)
    for l in range(layers):
        norm(l, acc[...])
        for g in range(chunks):
            project_kv(l, g)
            if l == 0 and g == 0:
                neighbours = sum(
                    jnp.where(there(dr, dc), 1, 0).astype(jnp.int32) for dr, dc in STEPS
                )
                pl.semaphore_wait(barrier, neighbours)
            send(l, g)
        project_q(l)
        if l == 0:
            fetch(0, ["o"])
            for later in range(1, layers):
                fetch(later, every + ["q", "o"])
            zero_missing()
            build_hidden()
            first[2].wait()
            build_flat()
        build_table(l)
        weight_copies[l, "o"].wait()
        receive_near(l, 0)
        for g in range(chunks):
            receive_far(l, g)
            if g + 1 < chunks:
                receive_near(l, g + 1)
            attend(l, g)
        acc[...] = acc[...].astype(jnp.bfloat16).astype(jnp.float32)
    out[...] = acc[...].astype(jnp.bfloat16).reshape(out.shape)
    for l in range(layers):
        for g in range(chunks):
            for d, (dr, dc) in enumerate(STEPS):
                @pl.when(direct(dr, dc))
                def _():
                    halo_copy(l, g, d).wait_send()

                if dr and dc:
                    @pl.when(relayed(dr, dc))
                    def _():
                        relay_copy(l, g, d).wait_send()


def on_device(sp_count, tp_count, grid_tokens, norm_gain, w_query, w_key, w_value, offset_bias, w_out):
    tile_rows, tile_cols, model_width = grid_tokens.shape
    layers, _, inner = w_query.shape
    tokens = tile_rows * tile_cols
    heads = inner // HEAD_DIM
    chunks = heads // CHUNK_HEADS
    part = CHUNK_HEADS * HEAD_DIM
    slab_rows = tile_rows + WIN_ROWS
    slab_cols = tile_cols + WIN_COLS
    slab = slab_rows * slab_cols
    flat_width = -(-(slab + tile_rows * slab_cols) // 128) * 128
    blocks = slab_cols // HALF_COLS
    bias_rows = jnp.transpose(offset_bias, (0, 2, 1, 3))
    bf16, f32 = jnp.bfloat16, jnp.float32
    hbm = pl.BlockSpec(memory_space=pltpu.HBM)
    return pl.pallas_call(
        functools.partial(kernel, sp_count=sp_count, tp_count=tp_count),
        out_shape=jax.ShapeDtypeStruct(grid_tokens.shape, bf16),
        in_specs=[hbm] * 7,
        out_specs=pl.BlockSpec(memory_space=pltpu.VMEM),
        scratch_shapes=[
            pltpu.VMEM(grid_tokens.shape, bf16),
            pltpu.VMEM(norm_gain.shape, f32),
            pltpu.VMEM(w_query.shape, bf16),
            pltpu.VMEM(w_key.shape, bf16),
            pltpu.VMEM(w_value.shape, bf16),
            pltpu.VMEM(w_out.shape, bf16),
            pltpu.VMEM(bias_rows.shape, f32),
            pltpu.VMEM((layers * heads, flat_width), f32),
            pltpu.VMEM((tile_cols, flat_width), f32),
            pltpu.VMEM((tokens, slab), f32),
            pltpu.VMEM((layers, heads, tokens, slab), f32),
            pltpu.VMEM((layers, chunks, slab_rows, blocks, HALF_COLS, 2 * part), bf16),
            pltpu.VMEM((tokens, model_width), bf16),
            pltpu.VMEM((tokens, inner), bf16),
            pltpu.VMEM((tokens, model_width), f32),
            pltpu.SemaphoreType.DMA((4,)),
            pltpu.SemaphoreType.DMA((layers, chunks, 2)),
            pltpu.SemaphoreType.DMA((layers, 2)),
            pltpu.SemaphoreType.DMA((layers, chunks, len(STEPS))),
            pltpu.SemaphoreType.DMA((layers, chunks, len(STEPS))),
        ],
        compiler_params=pltpu.CompilerParams(
            collective_id=0, has_side_effects=True, vmem_limit_bytes=54784 * 1024
        ),
    )(grid_tokens, pltpu.with_memory_space_constraint(norm_gain, pltpu.HBM), w_query, w_key, w_value, pltpu.with_memory_space_constraint(bias_rows, pltpu.HBM), w_out)


def solution(mesh):
    return jax.shard_map(
        functools.partial(on_device, mesh.shape["sp"], mesh.shape["tp"]),
        mesh=mesh,
        in_specs=(P(("grp", "sp"), "tp", None), P(), P(), P(), P(), P(), P()),
        out_specs=P(("grp", "sp"), "tp", None),
        check_vma=False,
    )
```

```python
import functools
import math

import jax
import jax.numpy as jnp
from jax import lax
from jax.experimental import pallas as pl
from jax.experimental.pallas import tpu as pltpu
from jax.sharding import PartitionSpec as P

HEAD_DIM = 128
WIN_ROWS = 8
WIN_COLS = 16
NORM_EPSILON = 1e-06
HALF_ROWS = WIN_ROWS // 2
HALF_COLS = WIN_COLS // 2
BELOW = WIN_ROWS - HALF_ROWS - 1
MESH = pl.DeviceIdType.MESH
LOG2E = math.log2(math.e)
HIDDEN = -1e30

KINDS = (
    "D_inner", "D_outer", "D_diag", "D_relay", "U_inner", "U_outer", "U_diag", "U_relay",
    "C_beside", "C_far",
)


def kernel(
    x_hbm, gain_hbm, wq_hbm, wk_hbm, wv_hbm, bias_hbm, wo_hbm, out,
    xs, ms, gain, wq, wk, wv, wo, bias, flat, wide, hidden, table, kv, queries, acc, tops, mixes,
    local_sem, w_sem, send_sem, recv_sem,
    *, sp_count, tp_count,
):
    layers, model_width, inner = wq.shape
    tile_rows, own_blocks = x_hbm.shape[:2]
    tile_cols = own_blocks * HALF_COLS
    tokens = tile_rows * tile_cols
    half = HALF_ROWS * tile_cols
    heads = inner // HEAD_DIM
    slab_rows = tile_rows + WIN_ROWS
    slab_cols = tile_cols + WIN_COLS
    slab = slab_rows * slab_cols
    edge = HALF_ROWS * slab_cols
    row_index = lax.axis_index("sp")
    col_index = lax.axis_index("tp")
    side = lax.rem(col_index, 2)
    beside, far = 1 - 2 * side, 2 * side - 1
    inner_block, outer_block = own_blocks - side * (own_blocks - 1), 1 + side * (own_blocks - 1)
    left_block, right_block = side * (own_blocks + 1), (1 - side) * (own_blocks + 1)

    has_above, has_below = row_index > 0, row_index < sp_count - 1
    has_beside = (col_index + beside >= 0) & (col_index + beside < tp_count)
    has_far = (col_index + far >= 0) & (col_index + far < tp_count)
    neighbours = (
        (-1, 0, has_above), (1, 0, has_below), (-1, far, has_above & has_far),
        (1, far, has_below & has_far), (0, far, has_far), (0, beside, has_beside),
    )

    own_rows = slice(HALF_ROWS, HALF_ROWS + tile_rows)
    own_cols = slice(1, 1 + own_blocks)
    every_block = slice(0, own_blocks + 2)
    above_rows = slice(0, HALF_ROWS)
    last_rows = slice(tile_rows, tile_rows + HALF_ROWS)
    first_rows = slice(HALF_ROWS, HALF_ROWS + BELOW)
    below_rows = slice(HALF_ROWS + tile_rows, HALF_ROWS + tile_rows + BELOW)
    OWN = ((own_rows, own_cols),)
    SIDES = ((own_rows, slice(0, 1)), (own_rows, slice(own_blocks + 1, own_blocks + 2)))
    EDGES = (
        (above_rows, every_block), (slice(slab_rows - HALF_ROWS, slab_rows), every_block),
    )

    barrier = pltpu.get_barrier_semaphore()
    for dr, dc, exists in neighbours:
        @pl.when(exists)
        def _():
            pl.semaphore_signal(
                barrier,
                inc=1,
                device_id={"sp": row_index + dr, "tp": col_index + dc},
                device_id_type=MESH,
            )

    first = [
        pltpu.make_async_copy(x_hbm, xs.at[own_rows, own_cols], local_sem.at[0]),
        pltpu.make_async_copy(gain_hbm, gain, local_sem.at[1]),
        pltpu.make_async_copy(bias_hbm, bias, local_sem.at[2]),
    ]
    for copy in first:
        copy.start()
    pairs = {"k": (wk_hbm, wk), "v": (wv_hbm, wv), "q": (wq_hbm, wq), "o": (wo_hbm, wo)}
    weight_copies = {}

    def fetch(l, names):
        for name in names:
            src, dst = pairs[name]
            copy = pltpu.make_async_copy(src.at[l], dst.at[l], w_sem.at[l, "kvqo".index(name)])
            copy.start()
            weight_copies[l, name] = copy

    def arrived(l, name):
        if (l, name) in weight_copies:
            weight_copies.pop((l, name)).wait()

    fetch(0, "kvq")

    def plan(kind):
        way, what = kind.split("_")
        if way == "C":
            if what == "beside":
                return own_rows, own_rows, inner_block, left_block, 0, beside, has_beside, has_beside
            return own_rows, own_rows, outer_block, right_block, 0, far, has_far, has_far
        dr = 1 if way == "D" else -1
        src_rows, dst_rows = (last_rows, above_rows) if dr == 1 else (first_rows, below_rows)
        goes, comes = (has_below, has_above) if dr == 1 else (has_above, has_below)
        if what == "inner":
            return src_rows, dst_rows, inner_block, inner_block, dr, 0, goes, comes
        if what == "outer":
            return src_rows, dst_rows, outer_block, outer_block, dr, 0, goes, comes
        if what == "diag":
            ends = outer_block, right_block
            return src_rows, dst_rows, *ends, dr, far, goes & has_far, comes & has_far
        passes = comes & has_beside
        return dst_rows, dst_rows, inner_block, left_block, 0, beside, passes, passes

    def halo_copy(l, kind):
        src_rows, dst_rows, src_block, dst_block, dr, dc, _, _ = plan(kind)
        ref = ms.at[l - 1] if l else xs
        i = KINDS.index(kind)
        return pltpu.make_async_remote_copy(
            src_ref=ref.at[src_rows, pl.ds(src_block, 1)],
            dst_ref=ref.at[dst_rows, pl.ds(dst_block, 1)],
            send_sem=send_sem.at[l, i],
            recv_sem=recv_sem.at[l, i],
            device_id={"sp": row_index + dr, "tp": col_index + dc},
            device_id_type=MESH,
        )

    def send(l, kinds):
        for kind in kinds:
            @pl.when(plan(kind)[6])
            def _():
                halo_copy(l, kind).start()

    def receive(l, kinds):
        for kind in kinds:
            @pl.when(plan(kind)[7])
            def _():
                halo_copy(l, kind).wait_recv()

    def pass_on(l, way):
        receive(l, [way + "_inner"])
        send(l, [way + "_relay"])

    def fill(rows, cols):
        for ref in [xs] + [ms.at[l] for l in range(layers - 1)]:
            shape = (rows.stop - rows.start, cols.stop - cols.start) + ref.shape[2:]
            ref[rows, cols] = jnp.zeros(shape, jnp.bfloat16)

    def zero_missing():
        received = slice(0, slab_rows - 1)
        fill(slice(slab_rows - 1, slab_rows), every_block)

        @pl.when(jnp.logical_not(has_above))
        def _():
            fill(above_rows, every_block)

        @pl.when(jnp.logical_not(has_below))
        def _():
            fill(below_rows, every_block)

        @pl.when(col_index == 0)
        def _():
            fill(received, slice(0, 1))

        @pl.when(col_index == tp_count - 1)
        def _():
            fill(received, slice(own_blocks + 1, own_blocks + 2))

    def gather(ref, pieces):
        width = ref.shape[-1]
        return jnp.concatenate(
            [ref[rows, cols].astype(jnp.float32).reshape(-1, width) for rows, cols in pieces]
        )

    def norm(l, stream):
        factor = lax.rsqrt(jnp.mean(stream * stream, axis=-1, keepdims=True) + NORM_EPSILON)
        return (stream * factor * gain[l : l + 1]).astype(jnp.bfloat16)

    def stream_of(l, pieces):
        stream = gather(xs, pieces)
        for done in range(l):
            mixture = gather(ms.at[done], pieces).astype(jnp.bfloat16)
            stream += jnp.dot(mixture, wo[done], preferred_element_type=jnp.float32)
            stream = stream.astype(jnp.bfloat16).astype(jnp.float32)
        return stream

    def project_kv(l, normed, pieces):
        for i, (name, w) in enumerate((("k", wk), ("v", wv))):
            arrived(l, name)
            made = jnp.dot(normed, w[l], preferred_element_type=jnp.float32)
            place = 0
            for rows, cols in pieces:
                shape = (rows.stop - rows.start, cols.stop - cols.start, HALF_COLS)
                count = math.prod(shape)
                kv[rows, cols, :, i * inner : (i + 1) * inner] = (
                    made[place : place + count].reshape(*shape, inner).astype(jnp.bfloat16)
                )
                place += count

    def project_q(l, normed):
        arrived(l, "q")
        made = jnp.dot(normed, wq[l], preferred_element_type=jnp.float32)
        queries[...] = (made * (LOG2E / HEAD_DIM**0.5)).astype(jnp.bfloat16)

    def prepare_own(l):
        normed = norm(l, acc[...])
        project_kv(l, normed, OWN)
        project_q(l, normed)

    def prepare(l, pieces):
        project_kv(l, norm(l, stream_of(l, pieces)), pieces)

    def build_hidden():
        k = lax.broadcasted_iota(jnp.int32, (1, slab), 1)
        key_row = k // slab_cols
        key_col = k - key_row * slab_cols
        row0 = row_index * tile_rows
        col0 = col_index * tile_cols
        c = lax.broadcasted_iota(jnp.int32, (tile_cols, 1), 0)
        col_start = jnp.clip(col0 + c - HALF_COLS, 0, tp_count * tile_cols - WIN_COLS)
        col_start = col_start - (col0 - HALF_COLS)
        col_inside = (key_col >= col_start) & (key_col < col_start + WIN_COLS)
        for r in range(tile_rows):
            start = jnp.clip(row0 + r - HALF_ROWS, 0, sp_count * tile_rows - WIN_ROWS)
            start = start - (row0 - HALF_ROWS)
            row_inside = (key_row >= start) & (key_row < start + WIN_ROWS)
            hidden[r * tile_cols : (r + 1) * tile_cols] = jnp.where(
                col_inside & row_inside, 0.0, HIDDEN
            )

    lead = tile_rows - 1 - BELOW

    def build_flat():
        row_count, col_count = 2 * WIN_ROWS - 1, 2 * WIN_COLS - 1
        flat[...] = jnp.zeros_like(flat)
        for l in range(layers):
            for a in range(row_count):
                place = (lead + a) * slab_cols
                flat[l * heads : (l + 1) * heads, place : place + col_count] = bias[l, a] * LOG2E

    def build_table(l):
        width = flat.shape[1]
        shift = (width - (WIN_COLS - 1 - HALF_COLS)) % width
        for h in range(heads):
            row = l * heads + h
            spread = jnp.broadcast_to(flat[row : row + 1, :], (tile_cols, width))
            wide[...] = pltpu.roll(spread, shift, 1, stride=1, stride_axis=0)
            for r in range(HALF_ROWS):
                first_lane = (tile_rows - 1 - r) * slab_cols
                seen = wide[:, first_lane : first_lane + slab - edge]
                for low in (0, edge):
                    start = r * tile_cols + (half if low else 0)
                    rows = slice(start, start + tile_cols)
                    keys = slice(low, low + slab - edge)
                    table[l, h, rows, keys] = seen + hidden[rows, keys]

    def keys_values(rows):
        count = (rows.stop - rows.start) * slab_cols
        return kv[rows].astype(jnp.float32).reshape(count, 2 * inner).astype(jnp.bfloat16)

    def score(l, h, span, keys, lanes):
        return lax.dot_general(
            queries[span, h * HEAD_DIM : (h + 1) * HEAD_DIM], keys,
            (((1,), (1,)), ((), ())), preferred_element_type=jnp.float32,
        ) + table[l, h, span, lanes]

    def weigh(expo, values):
        ones = jnp.ones(values.shape, jnp.bfloat16)
        return jnp.dot(
            expo, jnp.concatenate([values, ones], axis=1),
            preferred_element_type=jnp.float32,
        )

    def attend_own(l):
        both = keys_values(own_rows)
        for h in range(heads):
            keys = both[:, h * HEAD_DIM : (h + 1) * HEAD_DIM]
            values = both[:, inner + h * HEAD_DIM : inner + (h + 1) * HEAD_DIM]
            scores = score(l, h, slice(0, tokens), keys, slice(edge, slab - edge))
            top = jnp.max(scores, axis=1, keepdims=True)
            tops[h] = jnp.broadcast_to(top, (tokens, HEAD_DIM))
            mixes[h] = weigh(jnp.exp2(scores - top).astype(jnp.bfloat16), values)

    def attend_edges(l):
        both = jnp.concatenate([keys_values(rows) for rows, _ in EDGES])
        none = jnp.zeros((half, edge), jnp.bfloat16)
        mixture = []
        for h in range(heads):
            column = slice(h * HEAD_DIM, (h + 1) * HEAD_DIM)
            scores = lax.dot_general(
                queries[:, column], both[:, column],
                (((1,), (1,)), ((), ())), preferred_element_type=jnp.float32,
            )
            scores = jnp.concatenate([
                scores[:half, :edge] + table[l, h, :half, :edge],
                scores[half:, edge:] + table[l, h, half:, slab - edge :],
            ])
            top = jnp.maximum(tops[h], jnp.max(scores, axis=1, keepdims=True))
            scale = jnp.exp2(tops[h] - top)
            expo = jnp.exp2(scores - top).astype(jnp.bfloat16)
            expo = jnp.concatenate([
                jnp.concatenate([expo[:half], none], axis=1),
                jnp.concatenate([none, expo[half:]], axis=1),
            ])
            found = weigh(expo, both[:, inner + h * HEAD_DIM : inner + (h + 1) * HEAD_DIM])
            mix = mixes[h, :, :HEAD_DIM] * scale + found[:, :HEAD_DIM]
            total = mixes[h, :, HEAD_DIM:] * scale + found[:, HEAD_DIM:]
            mixture.append((mix / total).astype(jnp.bfloat16))
        return jnp.concatenate(mixture, axis=1)

    def finish(l, mixture):
        stream = acc[...] + jnp.dot(mixture, wo[l], preferred_element_type=jnp.float32)
        return stream.astype(jnp.bfloat16)

    zero_missing()
    first[0].wait()
    count = sum(jnp.where(exists, 1, 0).astype(jnp.int32) for _, _, exists in neighbours)
    pl.semaphore_wait(barrier, count)
    OUTGOING = [
        "D_inner", "U_inner", "C_far", "D_outer", "U_outer", "D_diag", "U_diag", "C_beside",
    ]
    send(0, OUTGOING)
    fetch(0, "o")
    for later in range(1, layers):
        fetch(later, "kvqo")
    first[1].wait()
    acc[...] = gather(xs, OWN)
    for l in range(layers):
        prepare_own(l)
        if l == 0:
            build_hidden()
            first[2].wait()
            build_flat()
        build_table(l)
        pass_on(l, "U")
        pass_on(l, "D")
        receive(l, ["C_beside", "C_far"])
        if l == 0:
            arrived(l, "o")
        prepare(l, SIDES)
        attend_own(l)
        receive(l, [way + what for way in "UD" for what in ("_outer", "_diag", "_relay")])
        prepare(l, EDGES)
        mixture = attend_edges(l)
        if l < layers - 1:
            ms[l, own_rows, own_cols] = (
                mixture.astype(jnp.float32)
                .reshape(tile_rows, own_blocks, HALF_COLS, inner)
                .astype(jnp.bfloat16)
            )
            send(l + 1, OUTGOING)
            acc[...] = finish(l, mixture).astype(jnp.float32)
        else:
            arrived(l, "o")
            out[...] = finish(l, mixture).reshape(out.shape)
    for l in range(layers):
        for kind in KINDS:
            @pl.when(plan(kind)[6])
            def _():
                halo_copy(l, kind).wait_send()


def on_device(sp_count, tp_count, grid_tokens, norm_gain, w_query, w_key, w_value, offset_bias, w_out):
    tile_rows, tile_cols, model_width = grid_tokens.shape
    layers, _, inner = w_query.shape
    tokens = tile_rows * tile_cols
    heads = inner // HEAD_DIM
    slab_rows = tile_rows + WIN_ROWS
    slab_cols = tile_cols + WIN_COLS
    slab = slab_rows * slab_cols
    flat_width = -(-(slab + tile_rows * slab_cols) // 128) * 128
    blocks = slab_cols // HALF_COLS
    bias_rows = jnp.transpose(offset_bias, (0, 2, 1, 3))
    blocked = grid_tokens.reshape(tile_rows, tile_cols // HALF_COLS, HALF_COLS, model_width)
    bf16, f32 = jnp.bfloat16, jnp.float32
    hbm = pl.BlockSpec(memory_space=pltpu.HBM)
    return pl.pallas_call(
        functools.partial(kernel, sp_count=sp_count, tp_count=tp_count),
        out_shape=jax.ShapeDtypeStruct(grid_tokens.shape, bf16),
        in_specs=[hbm] * 7,
        out_specs=pl.BlockSpec(memory_space=pltpu.VMEM),
        scratch_shapes=[
            pltpu.VMEM((slab_rows, blocks, HALF_COLS, model_width), bf16),
            pltpu.VMEM((max(layers - 1, 1), slab_rows, blocks, HALF_COLS, inner), bf16),
            pltpu.VMEM(norm_gain.shape, f32),
            pltpu.VMEM(w_query.shape, bf16),
            pltpu.VMEM(w_key.shape, bf16),
            pltpu.VMEM(w_value.shape, bf16),
            pltpu.VMEM(w_out.shape, bf16),
            pltpu.VMEM(bias_rows.shape, f32),
            pltpu.VMEM((layers * heads, flat_width), f32),
            pltpu.VMEM((tile_cols, flat_width), f32),
            pltpu.VMEM((tokens, slab), f32),
            pltpu.VMEM((layers, heads, tokens, slab), f32),
            pltpu.VMEM((slab_rows, blocks, HALF_COLS, 2 * inner), bf16),
            pltpu.VMEM((tokens, inner), bf16),
            pltpu.VMEM((tokens, model_width), f32),
            pltpu.VMEM((heads, tokens, HEAD_DIM), f32),
            pltpu.VMEM((heads, tokens, 2 * HEAD_DIM), f32),
            pltpu.SemaphoreType.DMA((3,)),
            pltpu.SemaphoreType.DMA((layers, 4)),
            pltpu.SemaphoreType.DMA((layers, len(KINDS))),
            pltpu.SemaphoreType.DMA((layers, len(KINDS))),
        ],
        compiler_params=pltpu.CompilerParams(
            collective_id=0, has_side_effects=True, vmem_limit_bytes=54784 * 1024
        ),
    )(
        blocked, pltpu.with_memory_space_constraint(norm_gain, pltpu.HBM), w_query, w_key,
        w_value, pltpu.with_memory_space_constraint(bias_rows, pltpu.HBM), w_out,
    )


def solution(mesh):
    return jax.shard_map(
        functools.partial(on_device, mesh.shape["sp"], mesh.shape["tp"]),
        mesh=mesh,
        in_specs=(P(("grp", "sp"), "tp", None), P(), P(), P(), P(), P(), P()),
        out_specs=P(("grp", "sp"), "tp", None),
        check_vma=False,
    )
```

```python
import functools
import math

import jax
import jax.numpy as jnp
from jax import lax
from jax.experimental import pallas as pl
from jax.experimental.pallas import tpu as pltpu
from jax.sharding import PartitionSpec as P

HEAD_DIM = 128
WIN_ROWS = 8
WIN_COLS = 16
NORM_EPSILON = 1e-06
HALF_ROWS = WIN_ROWS // 2
HALF_COLS = WIN_COLS // 2
BELOW = WIN_ROWS - HALF_ROWS - 1
MESH = pl.DeviceIdType.MESH
LOG2E = math.log2(math.e)
HIDDEN = -1e30

KINDS = (
    "D_inner", "D_outer", "D_diag", "D_relay", "U_inner", "U_outer", "U_diag", "U_relay",
    "C_beside", "C_far",
)


def kernel(
    x_hbm, gain_hbm, wq_hbm, wk_hbm, wv_hbm, bias_hbm, wo_hbm, out,
    xs, ms, gain, wq, wk, wv, wo, bias, flat, wide, hidden, table, kv, queries, acc, tops, mixes,
    local_sem, w_sem, send_sem, recv_sem,
    *, sp_count, tp_count,
):
    layers, model_width, inner = wq.shape
    tile_rows, own_blocks = x_hbm.shape[:2]
    tile_cols = own_blocks * HALF_COLS
    tokens = tile_rows * tile_cols
    half = HALF_ROWS * tile_cols
    heads = inner // HEAD_DIM
    slab_rows = tile_rows + WIN_ROWS
    slab_cols = tile_cols + WIN_COLS
    slab = slab_rows * slab_cols
    edge = HALF_ROWS * slab_cols
    row_index = lax.axis_index("sp")
    col_index = lax.axis_index("tp")
    side = lax.rem(col_index, 2)
    beside, far = 1 - 2 * side, 2 * side - 1
    inner_block, outer_block = own_blocks - side * (own_blocks - 1), 1 + side * (own_blocks - 1)
    left_block, right_block = side * (own_blocks + 1), (1 - side) * (own_blocks + 1)

    has_above, has_below = row_index > 0, row_index < sp_count - 1
    has_beside = (col_index + beside >= 0) & (col_index + beside < tp_count)
    has_far = (col_index + far >= 0) & (col_index + far < tp_count)
    neighbours = (
        (-1, 0, has_above), (1, 0, has_below), (-1, far, has_above & has_far),
        (1, far, has_below & has_far), (0, far, has_far), (0, beside, has_beside),
    )

    own_rows = slice(HALF_ROWS, HALF_ROWS + tile_rows)
    own_cols = slice(1, 1 + own_blocks)
    every_block = slice(0, own_blocks + 2)
    above_rows = slice(0, HALF_ROWS)
    last_rows = slice(tile_rows, tile_rows + HALF_ROWS)
    first_rows = slice(HALF_ROWS, HALF_ROWS + BELOW)
    below_rows = slice(HALF_ROWS + tile_rows, HALF_ROWS + tile_rows + BELOW)
    OWN = ((own_rows, own_cols),)
    SIDES = ((own_rows, slice(0, 1)), (own_rows, slice(own_blocks + 1, own_blocks + 2)))
    ABOVE = (above_rows, every_block)
    BENEATH = (slice(slab_rows - HALF_ROWS, slab_rows), every_block)
    EDGES = ABOVE, BENEATH

    barrier = pltpu.get_barrier_semaphore()
    for dr, dc, exists in neighbours:
        @pl.when(exists)
        def _():
            pl.semaphore_signal(
                barrier,
                inc=1,
                device_id={"sp": row_index + dr, "tp": col_index + dc},
                device_id_type=MESH,
            )

    first = [
        pltpu.make_async_copy(x_hbm, xs.at[own_rows, own_cols], local_sem.at[0]),
        pltpu.make_async_copy(gain_hbm, gain, local_sem.at[1]),
        pltpu.make_async_copy(bias_hbm, bias, local_sem.at[2]),
    ]
    for copy in first:
        copy.start()
    pairs = {"k": (wk_hbm, wk), "v": (wv_hbm, wv), "q": (wq_hbm, wq), "o": (wo_hbm, wo)}
    weight_copies = {}

    def fetch(l, names):
        for name in names:
            src, dst = pairs[name]
            copy = pltpu.make_async_copy(src.at[l], dst.at[l], w_sem.at[l, "kvqo".index(name)])
            copy.start()
            weight_copies[l, name] = copy

    def arrived(l, names):
        for name in names:
            weight_copies[l, name].wait()

    fetch(0, "kvq")

    def plan(kind):
        way, what = kind.split("_")
        if way == "C":
            if what == "beside":
                return own_rows, own_rows, inner_block, left_block, 0, beside, has_beside, has_beside
            return own_rows, own_rows, outer_block, right_block, 0, far, has_far, has_far
        dr = 1 if way == "D" else -1
        src_rows, dst_rows = (last_rows, above_rows) if dr == 1 else (first_rows, below_rows)
        goes, comes = (has_below, has_above) if dr == 1 else (has_above, has_below)
        if what == "inner":
            return src_rows, dst_rows, inner_block, inner_block, dr, 0, goes, comes
        if what == "outer":
            return src_rows, dst_rows, outer_block, outer_block, dr, 0, goes, comes
        if what == "diag":
            ends = outer_block, right_block
            return src_rows, dst_rows, *ends, dr, far, goes & has_far, comes & has_far
        passes = comes & has_beside
        return dst_rows, dst_rows, inner_block, left_block, 0, beside, passes, passes

    def halo_copy(l, kind):
        src_rows, dst_rows, src_block, dst_block, dr, dc, _, _ = plan(kind)
        ref = ms.at[l - 1] if l else xs
        i = KINDS.index(kind)
        return pltpu.make_async_remote_copy(
            src_ref=ref.at[src_rows, pl.ds(src_block, 1)],
            dst_ref=ref.at[dst_rows, pl.ds(dst_block, 1)],
            send_sem=send_sem.at[i],
            recv_sem=recv_sem.at[l, i],
            device_id={"sp": row_index + dr, "tp": col_index + dc},
            device_id_type=MESH,
        )

    def send(l, kinds):
        for kind in kinds:
            @pl.when(plan(kind)[6])
            def _():
                halo_copy(l, kind).start()

    def receive(l, kinds):
        for kind in kinds:
            @pl.when(plan(kind)[7])
            def _():
                halo_copy(l, kind).wait_recv()

    def sent(l):
        for kind in KINDS:
            @pl.when(plan(kind)[6])
            def _():
                halo_copy(l, kind).wait_send()

    def pass_on(l, way):
        receive(l, [way + "_inner"])
        send(l, [way + "_relay"])

    def zero(ref, rows, cols):
        shape = (rows.stop - rows.start, cols.stop - cols.start) + ref.shape[2:]
        ref[rows, cols] = jnp.zeros(shape, jnp.bfloat16)

    def zero_missing():
        exchanged = [xs] + [ms.at[l] for l in range(layers - 1)]
        for ref in exchanged:
            zero(ref, slice(slab_rows - 1, slab_rows), every_block)
        for exists, piece in ((has_above, ABOVE), (has_below, BENEATH)):
            @pl.when(jnp.logical_not(exists))
            def _():
                zero(kv, *piece)

        for block in (0, own_blocks + 1):
            @pl.when(col_index == (0 if block == 0 else tp_count - 1))
            def _():
                for ref in exchanged:
                    zero(ref, slice(0, slab_rows - 1), slice(block, block + 1))

    def gather(ref, pieces):
        width = ref.shape[-1]
        return jnp.concatenate(
            [ref[rows, cols].astype(jnp.float32).reshape(-1, width) for rows, cols in pieces]
        )

    def norm(l, stream):
        factor = lax.rsqrt(jnp.mean(stream * stream, axis=-1, keepdims=True) + NORM_EPSILON)
        return (stream * factor * gain[l : l + 1]).astype(jnp.bfloat16)

    def stream_of(l, pieces):
        stream = gather(xs, pieces)
        for done in range(l):
            mixture = gather(ms.at[done], pieces).astype(jnp.bfloat16)
            stream += jnp.dot(mixture, wo[done], preferred_element_type=jnp.float32)
            stream = stream.astype(jnp.bfloat16).astype(jnp.float32)
        return stream

    def project_kv(l, normed, pieces):
        for i, w in enumerate((wk, wv)):
            made = jnp.dot(normed, w[l], preferred_element_type=jnp.float32)
            place = 0
            for rows, cols in pieces:
                shape = (rows.stop - rows.start, cols.stop - cols.start, HALF_COLS)
                count = math.prod(shape)
                kv[rows, cols, :, i * inner : (i + 1) * inner] = (
                    made[place : place + count].reshape(*shape, inner).astype(jnp.bfloat16)
                )
                place += count

    def project_q(l, normed):
        made = jnp.dot(normed, wq[l], preferred_element_type=jnp.float32)
        queries[...] = (made * (LOG2E / HEAD_DIM**0.5)).astype(jnp.bfloat16)

    def prepare_own(l):
        normed = norm(l, acc[...])
        project_kv(l, normed, OWN)
        project_q(l, normed)

    def prepare(l, pieces):
        project_kv(l, norm(l, stream_of(l, pieces)), pieces)

    def build_hidden():
        k = lax.broadcasted_iota(jnp.int32, (1, slab), 1)
        key_row = k // slab_cols
        key_col = k - key_row * slab_cols
        row0 = row_index * tile_rows
        col0 = col_index * tile_cols
        c = lax.broadcasted_iota(jnp.int32, (tile_cols, 1), 0)
        col_start = jnp.clip(col0 + c - HALF_COLS, 0, tp_count * tile_cols - WIN_COLS)
        col_start = col_start - (col0 - HALF_COLS)
        col_inside = (key_col >= col_start) & (key_col < col_start + WIN_COLS)
        for r in range(tile_rows):
            start = jnp.clip(row0 + r - HALF_ROWS, 0, sp_count * tile_rows - WIN_ROWS)
            start = start - (row0 - HALF_ROWS)
            row_inside = (key_row >= start) & (key_row < start + WIN_ROWS)
            hidden[r * tile_cols : (r + 1) * tile_cols] = jnp.where(
                col_inside & row_inside, 0.0, HIDDEN
            )

    lead = tile_rows - 1 - BELOW

    def build_flat():
        row_count, col_count = 2 * WIN_ROWS - 1, 2 * WIN_COLS - 1
        flat[...] = jnp.zeros_like(flat)
        for l in range(layers):
            for a in range(row_count):
                place = (lead + a) * slab_cols
                flat[l * heads : (l + 1) * heads, place : place + col_count] = bias[l, a] * LOG2E

    def build_table(l):
        width = flat.shape[1]
        shift = (width - (WIN_COLS - 1 - HALF_COLS)) % width

        def one_head(h, carry):
            spread = jnp.broadcast_to(flat[pl.ds(l * heads + h, 1), :], (tile_cols, width))
            turned = pltpu.roll(spread, shift, 1, stride=1, stride_axis=0)
            for r in range(HALF_ROWS):
                first_lane = (tile_rows - 1 - r) * slab_cols
                seen = turned[:, first_lane : first_lane + slab - edge]
                for low in (0, edge):
                    start = r * tile_cols + (half if low else 0)
                    rows = slice(start, start + tile_cols)
                    keys = slice(low, low + slab - edge)
                    table[l, h, rows, keys] = seen + hidden[rows, keys]
            return carry

        lax.fori_loop(0, heads, one_head, 0)

    def keys_values(rows):
        count = (rows.stop - rows.start) * slab_cols
        return kv[rows].astype(jnp.float32).reshape(count, 2 * inner).astype(jnp.bfloat16)

    def score(l, h, span, keys, lanes):
        return lax.dot_general(
            queries[span, h * HEAD_DIM : (h + 1) * HEAD_DIM], keys,
            (((1,), (1,)), ((), ())), preferred_element_type=jnp.float32,
        ) + table[l, h, span, lanes]

    def weigh(expo, values):
        ones = jnp.ones(values.shape, jnp.bfloat16)
        return jnp.dot(
            expo, jnp.concatenate([values, ones], axis=1),
            preferred_element_type=jnp.float32,
        )

    def attend_own(l):
        both = keys_values(own_rows)
        for h in range(heads):
            keys = both[:, h * HEAD_DIM : (h + 1) * HEAD_DIM]
            values = both[:, inner + h * HEAD_DIM : inner + (h + 1) * HEAD_DIM]
            scores = score(l, h, slice(0, tokens), keys, slice(edge, slab - edge))
            top = jnp.max(scores, axis=1, keepdims=True)
            tops[h] = jnp.broadcast_to(top, (tokens, HEAD_DIM))
            mixes[h] = weigh(jnp.exp2(scores - top).astype(jnp.bfloat16), values)

    def attend_edges(l):
        both = jnp.concatenate([keys_values(rows) for rows, _ in EDGES])
        none = jnp.zeros((half, edge), jnp.bfloat16)
        mixture = []
        for h in range(heads):
            column = slice(h * HEAD_DIM, (h + 1) * HEAD_DIM)
            scores = lax.dot_general(
                queries[:, column], both[:, column],
                (((1,), (1,)), ((), ())), preferred_element_type=jnp.float32,
            )
            scores = jnp.concatenate([
                scores[:half, :edge] + table[l, h, :half, :edge],
                scores[half:, edge:] + table[l, h, half:, slab - edge :],
            ])
            top = jnp.maximum(tops[h], jnp.max(scores, axis=1, keepdims=True))
            scale = jnp.exp2(tops[h] - top)
            expo = jnp.exp2(scores - top).astype(jnp.bfloat16)
            expo = jnp.concatenate([
                jnp.concatenate([expo[:half], none], axis=1),
                jnp.concatenate([none, expo[half:]], axis=1),
            ])
            found = weigh(expo, both[:, inner + h * HEAD_DIM : inner + (h + 1) * HEAD_DIM])
            mix = mixes[h, :, :HEAD_DIM] * scale + found[:, :HEAD_DIM]
            total = mixes[h, :, HEAD_DIM:] * scale + found[:, HEAD_DIM:]
            mixture.append((mix / total).astype(jnp.bfloat16))
        return jnp.concatenate(mixture, axis=1)

    def finish(l, mixture):
        for low in range(0, model_width, 2 * HEAD_DIM):
            cols = slice(low, low + 2 * HEAD_DIM)
            stream = acc[:, cols] + jnp.dot(
                mixture, wo[l, :, cols], preferred_element_type=jnp.float32
            )
            stream = stream.astype(jnp.bfloat16)
            if l == layers - 1:
                out[:, :, cols] = stream.reshape(tile_rows, tile_cols, 2 * HEAD_DIM)
            else:
                acc[:, cols] = stream.astype(jnp.float32)

    zero_missing()
    first[0].wait()
    count = sum(jnp.where(exists, 1, 0).astype(jnp.int32) for _, _, exists in neighbours)
    pl.semaphore_wait(barrier, count)
    EARLY = ["C_beside", "D_inner", "U_inner", "C_far"]
    LATE = ["D_outer", "U_outer", "D_diag", "U_diag"]
    send(0, EARLY)
    fetch(0, "o")
    for later in range(1, layers):
        fetch(later, "kvqo")
    first[1].wait()
    acc[...] = gather(xs, OWN)
    for l in range(layers):
        if l == 0:
            arrived(0, "kvq")
        prepare_own(l)
        if l == 0:
            send(0, LATE)
            build_hidden()
            first[2].wait()
            build_flat()
        build_table(l)
        if l == 0:
            arrived(0, "o")
            for later in range(1, layers):
                arrived(later, "kvqo")
        pass_on(l, "U")
        pass_on(l, "D")
        receive(l, ["C_beside", "C_far"])
        prepare(l, SIDES)
        attend_own(l)
        receive(l, [way + what for way in "UD" for what in ("_outer", "_diag", "_relay")])
        if l == layers - 1:
            sent(l)
        for exist, pieces in (
            (has_above & has_below, EDGES),
            (has_above & jnp.logical_not(has_below), EDGES[:1]),
            (jnp.logical_not(has_above) & has_below, EDGES[1:]),
        ):
            @pl.when(exist)
            def _():
                prepare(l, pieces)
        mixture = attend_edges(l)
        if l < layers - 1:
            ms[l, own_rows, own_cols] = (
                mixture.astype(jnp.float32)
                .reshape(tile_rows, own_blocks, HALF_COLS, inner)
                .astype(jnp.bfloat16)
            )
            sent(l)
            send(l + 1, EARLY)
            finish(l, mixture)
            send(l + 1, LATE)
        else:
            finish(l, mixture)


def on_device(sp_count, tp_count, grid_tokens, norm_gain, w_query, w_key, w_value, offset_bias, w_out):
    tile_rows, tile_cols, model_width = grid_tokens.shape
    layers, _, inner = w_query.shape
    tokens = tile_rows * tile_cols
    heads = inner // HEAD_DIM
    slab_rows = tile_rows + WIN_ROWS
    slab_cols = tile_cols + WIN_COLS
    slab = slab_rows * slab_cols
    flat_width = -(-(slab + tile_rows * slab_cols) // 128) * 128
    blocks = slab_cols // HALF_COLS
    bias_rows = jnp.transpose(offset_bias, (0, 2, 1, 3))
    blocked = grid_tokens.reshape(tile_rows, tile_cols // HALF_COLS, HALF_COLS, model_width)
    bf16, f32 = jnp.bfloat16, jnp.float32
    hbm = pl.BlockSpec(memory_space=pltpu.HBM)
    return pl.pallas_call(
        functools.partial(kernel, sp_count=sp_count, tp_count=tp_count),
        out_shape=jax.ShapeDtypeStruct(grid_tokens.shape, bf16),
        in_specs=[hbm] * 7,
        out_specs=pl.BlockSpec(memory_space=pltpu.VMEM),
        scratch_shapes=[
            pltpu.VMEM((slab_rows, blocks, HALF_COLS, model_width), bf16),
            pltpu.VMEM((max(layers - 1, 1), slab_rows, blocks, HALF_COLS, inner), bf16),
            pltpu.VMEM(norm_gain.shape, f32),
            pltpu.VMEM(w_query.shape, bf16),
            pltpu.VMEM(w_key.shape, bf16),
            pltpu.VMEM(w_value.shape, bf16),
            pltpu.VMEM(w_out.shape, bf16),
            pltpu.VMEM(bias_rows.shape, f32),
            pltpu.VMEM((layers * heads, flat_width), f32),
            pltpu.VMEM((tile_cols, flat_width), f32),
            pltpu.VMEM((tokens, slab), f32),
            pltpu.VMEM((layers, heads, tokens, slab), f32),
            pltpu.VMEM((slab_rows, blocks, HALF_COLS, 2 * inner), bf16),
            pltpu.VMEM((tokens, inner), bf16),
            pltpu.VMEM((tokens, model_width), f32),
            pltpu.VMEM((heads, tokens, HEAD_DIM), f32),
            pltpu.VMEM((heads, tokens, 2 * HEAD_DIM), f32),
            pltpu.SemaphoreType.DMA((3,)),
            pltpu.SemaphoreType.DMA((layers, 4)),
            pltpu.SemaphoreType.DMA((len(KINDS),)),
            pltpu.SemaphoreType.DMA((layers, len(KINDS))),
        ],
        compiler_params=pltpu.CompilerParams(
            collective_id=0, has_side_effects=True, vmem_limit_bytes=54784 * 1024
        ),
    )(
        blocked, pltpu.with_memory_space_constraint(norm_gain, pltpu.HBM), w_query, w_key,
        w_value, pltpu.with_memory_space_constraint(bias_rows, pltpu.HBM), w_out,
    )


def solution(mesh):
    return jax.shard_map(
        functools.partial(on_device, mesh.shape["sp"], mesh.shape["tp"]),
        mesh=mesh,
        in_specs=(P(("grp", "sp"), "tp", None), P(), P(), P(), P(), P(), P()),
        out_specs=P(("grp", "sp"), "tp", None),
        check_vma=False,
    )
```

```python
import functools
import math

import jax
import jax.numpy as jnp
from jax import lax
from jax.experimental import pallas as pl
from jax.experimental.pallas import tpu as pltpu
from jax.sharding import PartitionSpec as P

HEAD_DIM = 128
WIN_ROWS = 8
WIN_COLS = 16
NORM_EPSILON = 1e-06
HALF_ROWS = WIN_ROWS // 2
HALF_COLS = WIN_COLS // 2
BELOW = WIN_ROWS - HALF_ROWS - 1
MESH = pl.DeviceIdType.MESH
LOG2E = math.log2(math.e)
HIDDEN = -1e30

KINDS = (
    "D_inner", "D_outer", "D_diag", "D_relay", "U_inner", "U_outer", "U_diag", "U_relay",
    "C_beside", "C_far",
)


def kernel(
    x_hbm, gain_hbm, wq_hbm, wk_hbm, wv_hbm, bias_hbm, wo_hbm, out,
    xs, ms, gain, wq, wk, wv, wo, bias, flat, wide, hidden, table, kv, queries, acc, tops, mixes,
    local_sem, w_sem, send_sem, recv_sem, entered_sem,
    *, sp_count, tp_count,
):
    layers, model_width, inner = wq.shape
    tile_rows, own_blocks = x_hbm.shape[:2]
    tile_cols = own_blocks * HALF_COLS
    tokens = tile_rows * tile_cols
    half = HALF_ROWS * tile_cols
    heads = inner // HEAD_DIM
    slab_rows = tile_rows + WIN_ROWS
    slab_cols = tile_cols + WIN_COLS
    slab = slab_rows * slab_cols
    edge = HALF_ROWS * slab_cols
    row_index = lax.axis_index("sp")
    col_index = lax.axis_index("tp")
    side = lax.rem(col_index, 2)
    beside, far = 1 - 2 * side, 2 * side - 1
    inner_block, outer_block = own_blocks - side * (own_blocks - 1), 1 + side * (own_blocks - 1)
    left_block, right_block = side * (own_blocks + 1), (1 - side) * (own_blocks + 1)

    has_above, has_below = row_index > 0, row_index < sp_count - 1
    has_beside = (col_index + beside >= 0) & (col_index + beside < tp_count)
    has_far = (col_index + far >= 0) & (col_index + far < tp_count)
    neighbours = (
        (-1, 0, has_above), (1, 0, has_below), (0, far, has_far), (0, beside, has_beside),
    )

    own_rows = slice(HALF_ROWS, HALF_ROWS + tile_rows)
    own_cols = slice(1, 1 + own_blocks)
    every_block = slice(0, own_blocks + 2)
    above_rows = slice(0, HALF_ROWS)
    last_rows = slice(tile_rows, tile_rows + HALF_ROWS)
    first_rows = slice(HALF_ROWS, HALF_ROWS + BELOW)
    below_rows = slice(HALF_ROWS + tile_rows, HALF_ROWS + tile_rows + BELOW)
    OWN = ((own_rows, own_cols),)
    BESIDE = (own_rows, pl.ds(right_block, 1))
    FAR = (own_rows, pl.ds(left_block, 1))
    ABOVE = (above_rows, every_block)
    BENEATH = (below_rows, every_block)
    EDGES = ABOVE, BENEATH

    barrier = pltpu.get_barrier_semaphore()
    for dr, dc, exists in neighbours:
        @pl.when(exists)
        def _():
            pl.semaphore_signal(
                barrier,
                inc=1,
                device_id={"sp": row_index + dr, "tp": col_index + dc},
                device_id_type=MESH,
            )

    first = [
        pltpu.make_async_copy(x_hbm, xs.at[own_rows, own_cols], local_sem.at[0]),
        pltpu.make_async_copy(gain_hbm, gain, local_sem.at[1]),
        pltpu.make_async_copy(bias_hbm, bias, local_sem.at[2]),
    ]
    for copy in first:
        copy.start()
    pairs = {"k": (wk_hbm, wk), "v": (wv_hbm, wv), "q": (wq_hbm, wq), "o": (wo_hbm, wo)}
    weight_copies = {}

    def fetch(l, names):
        for name in names:
            src, dst = pairs[name]
            copy = pltpu.make_async_copy(src.at[l], dst.at[l], w_sem.at[l, "kvqo".index(name)])
            copy.start()
            weight_copies[l, name] = copy

    def arrived(l, names):
        for name in names:
            weight_copies[l, name].wait()

    fetch(0, "kvq")

    def plan(kind):
        way, what = kind.split("_")
        if way == "C":
            if what == "beside":
                return own_rows, own_rows, inner_block, left_block, 0, beside, has_beside, has_beside
            return own_rows, own_rows, outer_block, right_block, 0, far, has_far, has_far
        dr = 1 if way == "D" else -1
        src_rows, dst_rows = (last_rows, above_rows) if dr == 1 else (first_rows, below_rows)
        goes, comes = (has_below, has_above) if dr == 1 else (has_above, has_below)
        if what == "inner":
            return src_rows, dst_rows, inner_block, inner_block, dr, 0, goes, comes
        if what == "outer":
            return src_rows, dst_rows, outer_block, outer_block, dr, 0, goes, comes
        if what == "diag":
            ends = outer_block, right_block
            return src_rows, dst_rows, *ends, dr, far, goes & has_far, comes & has_far
        passes = comes & has_beside
        return dst_rows, dst_rows, inner_block, left_block, 0, beside, passes, passes

    def halo_copy(l, kind):
        src_rows, dst_rows, src_block, dst_block, dr, dc, _, _ = plan(kind)
        ref = ms.at[l - 1] if l else xs
        i = KINDS.index(kind)
        return pltpu.make_async_remote_copy(
            src_ref=ref.at[src_rows, pl.ds(src_block, 1)],
            dst_ref=ref.at[dst_rows, pl.ds(dst_block, 1)],
            send_sem=send_sem.at[i],
            recv_sem=recv_sem.at[l, i],
            device_id={"sp": row_index + dr, "tp": col_index + dc},
            device_id_type=MESH,
        )

    def send(l, kinds):
        for kind in kinds:
            @pl.when(plan(kind)[6])
            def _():
                halo_copy(l, kind).start()

    def receive(l, kinds):
        for kind in kinds:
            @pl.when(plan(kind)[7])
            def _():
                halo_copy(l, kind).wait_recv()

    def sent(l):
        for kind in KINDS:
            @pl.when(plan(kind)[6])
            def _():
                halo_copy(l, kind).wait_send()

    def pass_on(l, way):
        receive(l, [way + "_inner"])
        send(l, [way + "_relay"])

    def shape_of(rows, cols):
        blocks = cols.size if isinstance(cols, pl.Slice) else cols.stop - cols.start
        return rows.stop - rows.start, blocks, HALF_COLS

    def zero(ref, rows, cols):
        shape = shape_of(rows, cols) + ref.shape[3:]
        ref[rows, cols] = jnp.zeros(shape, jnp.bfloat16)

    def zero_missing():
        exchanged = [xs] + [ms.at[l] for l in range(layers - 1)]
        zero(kv, slice(slab_rows - 1, slab_rows), every_block)
        for exists, piece in ((has_above, ABOVE), (has_below, BENEATH)):
            @pl.when(jnp.logical_not(exists))
            def _():
                zero(kv, *piece)

        @pl.when(jnp.logical_not(has_far))
        def _():
            zero(kv, *FAR)

        for block in (0, own_blocks + 1):
            @pl.when(col_index == (0 if block == 0 else tp_count - 1))
            def _():
                for ref in exchanged:
                    zero(ref, slice(0, slab_rows - 1), slice(block, block + 1))

    def gather(ref, pieces):
        width = ref.shape[-1]
        return jnp.concatenate(
            [ref[rows, cols].astype(jnp.float32).reshape(-1, width) for rows, cols in pieces]
        )

    def norm(l, stream):
        factor = lax.rsqrt(jnp.mean(stream * stream, axis=-1, keepdims=True) + NORM_EPSILON)
        return (stream * factor * gain[l : l + 1]).astype(jnp.bfloat16)

    def stream_of(l, pieces):
        stream = gather(xs, pieces)
        for done in range(l):
            mixture = gather(ms.at[done], pieces).astype(jnp.bfloat16)
            stream += jnp.dot(mixture, wo[done], preferred_element_type=jnp.float32)
            stream = stream.astype(jnp.bfloat16).astype(jnp.float32)
        return stream

    def project_kv(l, normed, pieces):
        for i, w in enumerate((wk, wv)):
            made = jnp.dot(normed, w[l], preferred_element_type=jnp.float32)
            place = 0
            for rows, cols in pieces:
                shape = shape_of(rows, cols)
                count = math.prod(shape)
                kv[rows, cols, :, i * inner : (i + 1) * inner] = (
                    made[place : place + count].reshape(*shape, inner).astype(jnp.bfloat16)
                )
                place += count

    def project_q(l, normed):
        made = jnp.dot(normed, wq[l], preferred_element_type=jnp.float32)
        queries[...] = (made * (LOG2E / HEAD_DIM**0.5)).astype(jnp.bfloat16)

    def prepare_own(l):
        normed = norm(l, acc[...])
        project_kv(l, normed, OWN)
        project_q(l, normed)

    def prepare(l, pieces):
        project_kv(l, norm(l, stream_of(l, pieces)), pieces)

    def build_hidden():
        k = lax.broadcasted_iota(jnp.int32, (1, slab), 1)
        key_row = k // slab_cols
        key_col = k - key_row * slab_cols
        row0 = row_index * tile_rows
        col0 = col_index * tile_cols
        c = lax.broadcasted_iota(jnp.int32, (tile_cols, 1), 0)
        col_start = jnp.clip(col0 + c - HALF_COLS, 0, tp_count * tile_cols - WIN_COLS)
        col_start = col_start - (col0 - HALF_COLS)
        col_inside = (key_col >= col_start) & (key_col < col_start + WIN_COLS)
        for r in range(tile_rows):
            start = jnp.clip(row0 + r - HALF_ROWS, 0, sp_count * tile_rows - WIN_ROWS)
            start = start - (row0 - HALF_ROWS)
            row_inside = (key_row >= start) & (key_row < start + WIN_ROWS)
            hidden[r * tile_cols : (r + 1) * tile_cols] = jnp.where(
                col_inside & row_inside, 0.0, HIDDEN
            )

    lead = tile_rows - 1 - BELOW

    def build_flat():
        row_count, col_count = 2 * WIN_ROWS - 1, 2 * WIN_COLS - 1
        flat[...] = jnp.zeros_like(flat)
        for l in range(layers):
            for a in range(row_count):
                place = (lead + a) * slab_cols
                flat[l * heads : (l + 1) * heads, place : place + col_count] = bias[l, a] * LOG2E

    def build_table(l):
        width = flat.shape[1]
        shift = (width - (WIN_COLS - 1 - HALF_COLS)) % width

        def one_head(h, carry):
            spread = jnp.broadcast_to(flat[pl.ds(l * heads + h, 1), :], (tile_cols, width))
            turned = pltpu.roll(spread, shift, 1, stride=1, stride_axis=0)
            for r in range(HALF_ROWS):
                first_lane = (tile_rows - 1 - r) * slab_cols
                seen = turned[:, first_lane : first_lane + slab - edge]
                for low in (0, edge):
                    start = r * tile_cols + (half if low else 0)
                    rows = slice(start, start + tile_cols)
                    keys = slice(low, low + slab - edge)
                    table[l, h, rows, keys] = seen + hidden[rows, keys]
            return carry

        lax.fori_loop(0, heads, one_head, 0)

    def keys_values(rows):
        count = (rows.stop - rows.start) * slab_cols
        return kv[rows].astype(jnp.float32).reshape(count, 2 * inner).astype(jnp.bfloat16)

    def score(l, h, span, keys, lanes):
        return lax.dot_general(
            queries[span, h * HEAD_DIM : (h + 1) * HEAD_DIM], keys,
            (((1,), (1,)), ((), ())), preferred_element_type=jnp.float32,
        ) + table[l, h, span, lanes]

    def weigh(expo, values):
        ones = jnp.ones(values.shape, jnp.bfloat16)
        return jnp.dot(
            expo, jnp.concatenate([values, ones], axis=1),
            preferred_element_type=jnp.float32,
        )

    def attend_own(l):
        both = keys_values(own_rows)
        for h in range(heads):
            keys = both[:, h * HEAD_DIM : (h + 1) * HEAD_DIM]
            values = both[:, inner + h * HEAD_DIM : inner + (h + 1) * HEAD_DIM]
            scores = score(l, h, slice(0, tokens), keys, slice(edge, slab - edge))
            top = jnp.max(scores, axis=1, keepdims=True)
            tops[h] = jnp.broadcast_to(top, (tokens, HEAD_DIM))
            mixes[h] = weigh(jnp.exp2(scores - top).astype(jnp.bfloat16), values)

    def attend_edges(l):
        beyond = above_rows, slice(slab_rows - HALF_ROWS, slab_rows)
        both = jnp.concatenate([keys_values(rows) for rows in beyond])
        none = jnp.zeros((half, edge), jnp.bfloat16)
        mixture = []
        for h in range(heads):
            column = slice(h * HEAD_DIM, (h + 1) * HEAD_DIM)
            scores = lax.dot_general(
                queries[:, column], both[:, column],
                (((1,), (1,)), ((), ())), preferred_element_type=jnp.float32,
            )
            scores = jnp.concatenate([
                scores[:half, :edge] + table[l, h, :half, :edge],
                scores[half:, edge:] + table[l, h, half:, slab - edge :],
            ])
            top = jnp.maximum(tops[h], jnp.max(scores, axis=1, keepdims=True))
            scale = jnp.exp2(tops[h] - top)
            expo = jnp.exp2(scores - top).astype(jnp.bfloat16)
            expo = jnp.concatenate([
                jnp.concatenate([expo[:half], none], axis=1),
                jnp.concatenate([none, expo[half:]], axis=1),
            ])
            found = weigh(expo, both[:, inner + h * HEAD_DIM : inner + (h + 1) * HEAD_DIM])
            mix = mixes[h, :, :HEAD_DIM] * scale + found[:, :HEAD_DIM]
            total = mixes[h, :, HEAD_DIM:] * scale + found[:, HEAD_DIM:]
            mixture.append((mix / total).astype(jnp.bfloat16))
        return jnp.concatenate(mixture, axis=1)

    def finish(l, mixture):
        for low in range(0, model_width, 2 * HEAD_DIM):
            cols = slice(low, low + 2 * HEAD_DIM)
            stream = acc[:, cols] + jnp.dot(
                mixture, wo[l, :, cols], preferred_element_type=jnp.float32
            )
            stream = stream.astype(jnp.bfloat16)
            if l == layers - 1:
                out[:, :, cols] = stream.reshape(tile_rows, tile_cols, 2 * HEAD_DIM)
            else:
                acc[:, cols] = stream.astype(jnp.float32)

    zero_missing()
    first[0].wait()
    count = sum(jnp.where(exists, 1, 0).astype(jnp.int32) for _, _, exists in neighbours)
    pl.semaphore_wait(barrier, count)
    EARLY = ["C_beside", "D_inner", "U_inner", "C_far"]
    OUTER, DIAG = ["D_outer", "U_outer"], ["D_diag", "U_diag"]
    send(0, EARLY)
    for way, (dr, exists) in enumerate(((-1, has_above), (1, has_below))):
        @pl.when(exists & has_far)
        def _():
            pl.semaphore_signal(
                entered_sem.at[way],
                inc=1,
                device_id={"sp": row_index + dr, "tp": col_index},
                device_id_type=MESH,
            )
    fetch(0, "o")
    for later in range(1, layers):
        fetch(later, "kvqo")
    first[1].wait()
    acc[...] = gather(xs, OWN)
    for l in range(layers):
        if l == 0:
            arrived(0, "kvq")
            send(0, OUTER)
        prepare_own(l)
        if l == 0:
            for way, exists in enumerate((has_below, has_above)):
                @pl.when(exists & has_far)
                def _():
                    pl.semaphore_wait(entered_sem.at[way], 1)

            send(0, DIAG)
            build_hidden()
            first[2].wait()
            build_flat()
        build_table(l)
        if l == 0:
            arrived(0, "o")
            for later in range(1, layers):
                arrived(later, "kvqo")
        receive(l, ["C_beside"])
        prepare(l, (BESIDE,))

        @pl.when(jnp.logical_not(has_far))
        def _():
            attend_own(l)

        pass_on(l, "U")
        pass_on(l, "D")
        receive(l, ["C_far"])

        @pl.when(has_far)
        def _():
            prepare(l, (FAR,))
            attend_own(l)

        arrivals = {
            way: [way + "_" + what for what in ("outer", "diag", "relay")] for way in "UD"
        }
        if l == 0:
            for way, exists, piece in (("U", has_below, BENEATH), ("D", has_above, ABOVE)):
                receive(l, arrivals[way])

                @pl.when(exists)
                def _():
                    prepare(l, (piece,))
        else:
            receive(l, arrivals["U"] + arrivals["D"])
            for exist, pieces in (
                (has_above & has_below, EDGES),
                (has_above & jnp.logical_not(has_below), EDGES[:1]),
                (jnp.logical_not(has_above) & has_below, EDGES[1:]),
            ):
                @pl.when(exist)
                def _():
                    prepare(l, pieces)
        if l == layers - 1:
            sent(l)
        mixture = attend_edges(l)
        if l < layers - 1:
            ms[l, own_rows, own_cols] = (
                mixture.astype(jnp.float32)
                .reshape(tile_rows, own_blocks, HALF_COLS, inner)
                .astype(jnp.bfloat16)
            )
            sent(l)
            send(l + 1, EARLY)
            finish(l, mixture)
            send(l + 1, OUTER + DIAG)
        else:
            finish(l, mixture)


def on_device(sp_count, tp_count, grid_tokens, norm_gain, w_query, w_key, w_value, offset_bias, w_out):
    tile_rows, tile_cols, model_width = grid_tokens.shape
    layers, _, inner = w_query.shape
    tokens = tile_rows * tile_cols
    heads = inner // HEAD_DIM
    slab_rows = tile_rows + WIN_ROWS
    slab_cols = tile_cols + WIN_COLS
    slab = slab_rows * slab_cols
    flat_width = -(-(slab + tile_rows * slab_cols) // 128) * 128
    blocks = slab_cols // HALF_COLS
    bias_rows = jnp.transpose(offset_bias, (0, 2, 1, 3))
    blocked = grid_tokens.reshape(tile_rows, tile_cols // HALF_COLS, HALF_COLS, model_width)
    bf16, f32 = jnp.bfloat16, jnp.float32
    hbm = pl.BlockSpec(memory_space=pltpu.HBM)
    return pl.pallas_call(
        functools.partial(kernel, sp_count=sp_count, tp_count=tp_count),
        out_shape=jax.ShapeDtypeStruct(grid_tokens.shape, bf16),
        in_specs=[hbm] * 7,
        out_specs=pl.BlockSpec(memory_space=pltpu.VMEM),
        scratch_shapes=[
            pltpu.VMEM((slab_rows, blocks, HALF_COLS, model_width), bf16),
            pltpu.VMEM((max(layers - 1, 1), slab_rows, blocks, HALF_COLS, inner), bf16),
            pltpu.VMEM(norm_gain.shape, f32),
            pltpu.VMEM(w_query.shape, bf16),
            pltpu.VMEM(w_key.shape, bf16),
            pltpu.VMEM(w_value.shape, bf16),
            pltpu.VMEM(w_out.shape, bf16),
            pltpu.VMEM(bias_rows.shape, f32),
            pltpu.VMEM((layers * heads, flat_width), f32),
            pltpu.VMEM((tile_cols, flat_width), f32),
            pltpu.VMEM((tokens, slab), f32),
            pltpu.VMEM((layers, heads, tokens, slab), f32),
            pltpu.VMEM((slab_rows, blocks, HALF_COLS, 2 * inner), bf16),
            pltpu.VMEM((tokens, inner), bf16),
            pltpu.VMEM((tokens, model_width), f32),
            pltpu.VMEM((heads, tokens, HEAD_DIM), f32),
            pltpu.VMEM((heads, tokens, 2 * HEAD_DIM), f32),
            pltpu.SemaphoreType.DMA((3,)),
            pltpu.SemaphoreType.DMA((layers, 4)),
            pltpu.SemaphoreType.DMA((len(KINDS),)),
            pltpu.SemaphoreType.DMA((layers, len(KINDS))),
            pltpu.SemaphoreType.REGULAR((2,)),
        ],
        compiler_params=pltpu.CompilerParams(
            collective_id=0, has_side_effects=True, vmem_limit_bytes=54784 * 1024
        ),
    )(
        blocked, pltpu.with_memory_space_constraint(norm_gain, pltpu.HBM), w_query, w_key,
        w_value, pltpu.with_memory_space_constraint(bias_rows, pltpu.HBM), w_out,
    )


def solution(mesh):
    return jax.shard_map(
        functools.partial(on_device, mesh.shape["sp"], mesh.shape["tp"]),
        mesh=mesh,
        in_specs=(P(("grp", "sp"), "tp", None), P(), P(), P(), P(), P(), P()),
        out_specs=P(("grp", "sp"), "tp", None),
        check_vma=False,
    )
```

```python
import functools
import math

import jax
import jax.numpy as jnp
from jax import lax
from jax.experimental import pallas as pl
from jax.experimental.pallas import tpu as pltpu
from jax.sharding import PartitionSpec as P

HEAD_DIM = 128
WIN_ROWS = 8
WIN_COLS = 16
NORM_EPSILON = 1e-06
HALF_ROWS = WIN_ROWS // 2
HALF_COLS = WIN_COLS // 2
BELOW = WIN_ROWS - HALF_ROWS - 1
MESH = pl.DeviceIdType.MESH
LOG2E = math.log2(math.e)
HIDDEN = -1e30

KINDS = (
    "D_inner", "D_outer", "D_diag", "D_relay", "U_inner", "U_outer", "U_diag", "U_relay",
    "C_beside", "C_far",
)


def kernel(
    x_hbm, gain_hbm, wq_hbm, wk_hbm, wv_hbm, bias_hbm, wo_hbm, out,
    xs, ms, gain, wq, wk, wv, wo, bias, flat, wide, hidden, table, kv, queries, acc, tops, mixes,
    local_sem, w_sem, send_sem, recv_sem, entered_sem,
    *, sp_count, tp_count,
):
    layers, model_width, inner = wq.shape
    tile_rows, own_blocks = x_hbm.shape[:2]
    tile_cols = own_blocks * HALF_COLS
    tokens = tile_rows * tile_cols
    half = HALF_ROWS * tile_cols
    heads = inner // HEAD_DIM
    slab_rows = tile_rows + WIN_ROWS
    slab_cols = tile_cols + WIN_COLS
    slab = slab_rows * slab_cols
    edge = HALF_ROWS * slab_cols
    row_index = lax.axis_index("sp")
    col_index = lax.axis_index("tp")
    side = lax.rem(col_index, 2)
    beside, far = 1 - 2 * side, 2 * side - 1
    inner_block, outer_block = own_blocks - side * (own_blocks - 1), 1 + side * (own_blocks - 1)
    left_block, right_block = side * (own_blocks + 1), (1 - side) * (own_blocks + 1)

    has_above, has_below = row_index > 0, row_index < sp_count - 1
    has_beside = (col_index + beside >= 0) & (col_index + beside < tp_count)
    has_far = (col_index + far >= 0) & (col_index + far < tp_count)
    neighbours = (
        (-1, 0, has_above), (1, 0, has_below), (0, far, has_far), (0, beside, has_beside),
    )

    own_rows = slice(HALF_ROWS, HALF_ROWS + tile_rows)
    own_cols = slice(1, 1 + own_blocks)
    every_block = slice(0, own_blocks + 2)
    above_rows = slice(0, HALF_ROWS)
    last_rows = slice(tile_rows, tile_rows + HALF_ROWS)
    first_rows = slice(HALF_ROWS, HALF_ROWS + BELOW)
    below_rows = slice(HALF_ROWS + tile_rows, HALF_ROWS + tile_rows + BELOW)
    OWN = ((own_rows, own_cols),)
    BESIDE = (own_rows, pl.ds(right_block, 1))
    FAR = (own_rows, pl.ds(left_block, 1))
    ABOVE = (above_rows, every_block)
    BENEATH = (below_rows, every_block)
    EDGES = ABOVE, BENEATH

    barrier = pltpu.get_barrier_semaphore()
    for dr, dc, exists in neighbours:
        @pl.when(exists)
        def _():
            pl.semaphore_signal(
                barrier,
                inc=1,
                device_id={"sp": row_index + dr, "tp": col_index + dc},
                device_id_type=MESH,
            )

    first = [
        pltpu.make_async_copy(x_hbm, xs.at[own_rows, own_cols], local_sem.at[0]),
        pltpu.make_async_copy(gain_hbm, gain, local_sem.at[1]),
        pltpu.make_async_copy(bias_hbm, bias, local_sem.at[2]),
    ]
    for copy in first:
        copy.start()
    pairs = {"k": (wk_hbm, wk), "v": (wv_hbm, wv), "q": (wq_hbm, wq), "o": (wo_hbm, wo)}
    weight_copies = {}

    def fetch(l, names):
        for name in names:
            src, dst = pairs[name]
            copy = pltpu.make_async_copy(src.at[l], dst.at[l], w_sem.at[l, "kvqo".index(name)])
            copy.start()
            weight_copies[l, name] = copy

    def arrived(l, names):
        for name in names:
            weight_copies[l, name].wait()

    fetch(0, "kvq")

    def plan(kind):
        way, what = kind.split("_")
        if way == "C":
            if what == "beside":
                return own_rows, own_rows, inner_block, left_block, 0, beside, has_beside, has_beside
            return own_rows, own_rows, outer_block, right_block, 0, far, has_far, has_far
        dr = 1 if way == "D" else -1
        src_rows, dst_rows = (last_rows, above_rows) if dr == 1 else (first_rows, below_rows)
        goes, comes = (has_below, has_above) if dr == 1 else (has_above, has_below)
        if what == "inner":
            return src_rows, dst_rows, inner_block, inner_block, dr, 0, goes, comes
        if what == "outer":
            return src_rows, dst_rows, outer_block, outer_block, dr, 0, goes, comes
        if what == "diag":
            ends = outer_block, right_block
            return src_rows, dst_rows, *ends, dr, far, goes & has_far, comes & has_far
        passes = comes & has_beside
        return dst_rows, dst_rows, inner_block, left_block, 0, beside, passes, passes

    def halo_copy(l, kind):
        src_rows, dst_rows, src_block, dst_block, dr, dc, _, _ = plan(kind)
        ref = ms.at[l - 1] if l else xs
        i = KINDS.index(kind)
        return pltpu.make_async_remote_copy(
            src_ref=ref.at[src_rows, pl.ds(src_block, 1)],
            dst_ref=ref.at[dst_rows, pl.ds(dst_block, 1)],
            send_sem=send_sem.at[i],
            recv_sem=recv_sem.at[l, i],
            device_id={"sp": row_index + dr, "tp": col_index + dc},
            device_id_type=MESH,
        )

    def send(l, kinds):
        for kind in kinds:
            @pl.when(plan(kind)[6])
            def _():
                halo_copy(l, kind).start()

    def receive(l, kinds):
        for kind in kinds:
            @pl.when(plan(kind)[7])
            def _():
                halo_copy(l, kind).wait_recv()

    def sent(l):
        for kind in KINDS:
            @pl.when(plan(kind)[6])
            def _():
                halo_copy(l, kind).wait_send()

    def pass_on(l, way):
        receive(l, [way + "_inner"])
        send(l, [way + "_relay"])

    def shape_of(rows, cols):
        blocks = cols.size if isinstance(cols, pl.Slice) else cols.stop - cols.start
        return rows.stop - rows.start, blocks, HALF_COLS

    def zero(ref, rows, cols):
        shape = shape_of(rows, cols) + ref.shape[3:]
        ref[rows, cols] = jnp.zeros(shape, jnp.bfloat16)

    def zero_missing():
        exchanged = [xs] + [ms.at[l] for l in range(layers - 1)]
        zero(kv, slice(slab_rows - 1, slab_rows), every_block)
        for exists, piece in ((has_above, ABOVE), (has_below, BENEATH)):
            @pl.when(jnp.logical_not(exists))
            def _():
                zero(kv, *piece)

        @pl.when(jnp.logical_not(has_far))
        def _():
            zero(kv, *FAR)

        for block in (0, own_blocks + 1):
            @pl.when(col_index == (0 if block == 0 else tp_count - 1))
            def _():
                for ref in exchanged:
                    zero(ref, slice(0, slab_rows - 1), slice(block, block + 1))

    def gather(ref, pieces):
        width = ref.shape[-1]
        return jnp.concatenate(
            [ref[rows, cols].astype(jnp.float32).reshape(-1, width) for rows, cols in pieces]
        )

    def norm(l, stream):
        factor = lax.rsqrt(jnp.mean(stream * stream, axis=-1, keepdims=True) + NORM_EPSILON)
        return (stream * gain[l : l + 1]).astype(jnp.bfloat16), factor

    def stream_of(l, pieces):
        stream = gather(xs, pieces)
        for done in range(l):
            mixture = gather(ms.at[done], pieces).astype(jnp.bfloat16)
            stream += jnp.dot(mixture, wo[done], preferred_element_type=jnp.float32)
            stream = stream.astype(jnp.bfloat16).astype(jnp.float32)
        return stream

    def project_kv(l, normed, pieces):
        scaled, factor = normed
        for i, w in enumerate((wk, wv)):
            made = jnp.dot(scaled, w[l], preferred_element_type=jnp.float32) * factor
            place = 0
            for rows, cols in pieces:
                shape = shape_of(rows, cols)
                count = math.prod(shape)
                kv[rows, cols, :, i * inner : (i + 1) * inner] = (
                    made[place : place + count].reshape(*shape, inner).astype(jnp.bfloat16)
                )
                place += count

    def project_q(l, normed):
        scaled, factor = normed
        made = jnp.dot(scaled, wq[l], preferred_element_type=jnp.float32)
        queries[...] = (made * (factor * (LOG2E / HEAD_DIM**0.5))).astype(jnp.bfloat16)

    def prepare_own(l):
        normed = norm(l, acc[...])
        project_kv(l, normed, OWN)
        project_q(l, normed)

    def prepare(l, pieces):
        project_kv(l, norm(l, stream_of(l, pieces)), pieces)

    def build_hidden():
        k = lax.broadcasted_iota(jnp.int32, (1, slab), 1)
        key_row = k // slab_cols
        key_col = k - key_row * slab_cols
        row0 = row_index * tile_rows
        col0 = col_index * tile_cols
        c = lax.broadcasted_iota(jnp.int32, (tile_cols, 1), 0)
        col_start = jnp.clip(col0 + c - HALF_COLS, 0, tp_count * tile_cols - WIN_COLS)
        col_start = col_start - (col0 - HALF_COLS)
        col_inside = (key_col >= col_start) & (key_col < col_start + WIN_COLS)
        for r in range(tile_rows):
            start = jnp.clip(row0 + r - HALF_ROWS, 0, sp_count * tile_rows - WIN_ROWS)
            start = start - (row0 - HALF_ROWS)
            row_inside = (key_row >= start) & (key_row < start + WIN_ROWS)
            hidden[r * tile_cols : (r + 1) * tile_cols] = jnp.where(
                col_inside & row_inside, 0.0, HIDDEN
            )

    lead = tile_rows - 1 - BELOW

    def build_flat():
        row_count, col_count = 2 * WIN_ROWS - 1, 2 * WIN_COLS - 1
        flat[...] = jnp.zeros_like(flat)
        for l in range(layers):
            for a in range(row_count):
                place = (lead + a) * slab_cols
                flat[l * heads : (l + 1) * heads, place : place + col_count] = bias[l, a] * LOG2E

    def build_table(l):
        width = flat.shape[1]
        shift = (width - (WIN_COLS - 1 - HALF_COLS)) % width

        def one_head(h, carry):
            spread = jnp.broadcast_to(flat[pl.ds(l * heads + h, 1), :], (tile_cols, width))
            turned = pltpu.roll(spread, shift, 1, stride=1, stride_axis=0)
            for r in range(HALF_ROWS):
                first_lane = (tile_rows - 1 - r) * slab_cols
                seen = turned[:, first_lane : first_lane + slab - edge]
                for low in (0, edge):
                    start = r * tile_cols + (half if low else 0)
                    rows = slice(start, start + tile_cols)
                    keys = slice(low, low + slab - edge)
                    table[l, h, rows, keys] = seen + hidden[rows, keys]
            return carry

        lax.fori_loop(0, heads, one_head, 0)

    def keys_values(rows):
        count = (rows.stop - rows.start) * slab_cols
        return kv[rows].astype(jnp.float32).reshape(count, 2 * inner).astype(jnp.bfloat16)

    def score(l, h, span, keys, lanes):
        return lax.dot_general(
            queries[span, h * HEAD_DIM : (h + 1) * HEAD_DIM], keys,
            (((1,), (1,)), ((), ())), preferred_element_type=jnp.float32,
        ) + table[l, h, span, lanes]

    def weigh(expo, values):
        ones = jnp.ones(values.shape, jnp.bfloat16)
        return jnp.dot(
            expo, jnp.concatenate([values, ones], axis=1),
            preferred_element_type=jnp.float32,
        )

    def attend_own(l):
        both = keys_values(own_rows)
        for h in range(heads):
            keys = both[:, h * HEAD_DIM : (h + 1) * HEAD_DIM]
            values = both[:, inner + h * HEAD_DIM : inner + (h + 1) * HEAD_DIM]
            scores = score(l, h, slice(0, tokens), keys, slice(edge, slab - edge))
            top = jnp.max(scores, axis=1, keepdims=True)
            tops[h] = jnp.broadcast_to(top, (tokens, HEAD_DIM))
            mixes[h] = weigh(jnp.exp2(scores - top).astype(jnp.bfloat16), values)

    def attend_edges(l):
        beyond = above_rows, slice(slab_rows - HALF_ROWS, slab_rows)
        both = jnp.concatenate([keys_values(rows) for rows in beyond])
        none = jnp.zeros((half, edge), jnp.bfloat16)
        mixture = []
        for h in range(heads):
            column = slice(h * HEAD_DIM, (h + 1) * HEAD_DIM)
            scores = lax.dot_general(
                queries[:, column], both[:, column],
                (((1,), (1,)), ((), ())), preferred_element_type=jnp.float32,
            )
            scores = jnp.concatenate([
                scores[:half, :edge] + table[l, h, :half, :edge],
                scores[half:, edge:] + table[l, h, half:, slab - edge :],
            ])
            top = jnp.maximum(tops[h], jnp.max(scores, axis=1, keepdims=True))
            scale = jnp.exp2(tops[h] - top)
            expo = jnp.exp2(scores - top).astype(jnp.bfloat16)
            expo = jnp.concatenate([
                jnp.concatenate([expo[:half], none], axis=1),
                jnp.concatenate([none, expo[half:]], axis=1),
            ])
            found = weigh(expo, both[:, inner + h * HEAD_DIM : inner + (h + 1) * HEAD_DIM])
            mix = mixes[h, :, :HEAD_DIM] * scale + found[:, :HEAD_DIM]
            total = mixes[h, :, HEAD_DIM:] * scale + found[:, HEAD_DIM:]
            mixture.append((mix / total).astype(jnp.bfloat16))
        return jnp.concatenate(mixture, axis=1)

    def finish(l, mixture):
        for low in range(0, model_width, 2 * HEAD_DIM):
            cols = slice(low, low + 2 * HEAD_DIM)
            stream = acc[:, cols] + jnp.dot(
                mixture, wo[l, :, cols], preferred_element_type=jnp.float32
            )
            stream = stream.astype(jnp.bfloat16)
            if l == layers - 1:
                out[:, :, cols] = stream.reshape(tile_rows, tile_cols, 2 * HEAD_DIM)
            else:
                acc[:, cols] = stream.astype(jnp.float32)

    zero_missing()
    first[0].wait()
    count = sum(jnp.where(exists, 1, 0).astype(jnp.int32) for _, _, exists in neighbours)
    pl.semaphore_wait(barrier, count)
    EARLY = ["C_beside", "D_inner", "U_inner", "C_far"]
    OUTER, DIAG = ["D_outer", "U_outer"], ["D_diag", "U_diag"]
    send(0, EARLY)
    for way, (dr, exists) in enumerate(((-1, has_above), (1, has_below))):
        @pl.when(exists & has_far)
        def _():
            pl.semaphore_signal(
                entered_sem.at[way],
                inc=1,
                device_id={"sp": row_index + dr, "tp": col_index},
                device_id_type=MESH,
            )
    fetch(0, "o")
    for later in range(1, layers):
        fetch(later, "kvqo")
    first[1].wait()
    acc[...] = gather(xs, OWN)
    for l in range(layers):
        if l == 0:
            arrived(0, "kvq")
            send(0, OUTER)
        prepare_own(l)
        if l == 0:
            for way, exists in enumerate((has_below, has_above)):
                @pl.when(exists & has_far)
                def _():
                    pl.semaphore_wait(entered_sem.at[way], 1)

            send(0, DIAG)
            build_hidden()
            first[2].wait()
            build_flat()
        build_table(l)
        if l == 0:
            arrived(0, "o")
            for later in range(1, layers):
                arrived(later, "kvqo")
        receive(l, ["C_beside"])
        prepare(l, (BESIDE,))

        @pl.when(jnp.logical_not(has_far))
        def _():
            attend_own(l)

        pass_on(l, "U")
        pass_on(l, "D")
        receive(l, ["C_far"])

        @pl.when(has_far)
        def _():
            prepare(l, (FAR,))
            attend_own(l)

        arrivals = {
            way: [way + "_" + what for what in ("outer", "diag", "relay")] for way in "UD"
        }
        if l == 0:
            for way, exists, piece in (("D", has_above, ABOVE), ("U", has_below, BENEATH)):
                receive(l, arrivals[way])

                @pl.when(exists)
                def _():
                    prepare(l, (piece,))
        else:
            receive(l, arrivals["U"] + arrivals["D"])
            for exist, pieces in (
                (has_above & has_below, EDGES),
                (has_above & jnp.logical_not(has_below), EDGES[:1]),
                (jnp.logical_not(has_above) & has_below, EDGES[1:]),
            ):
                @pl.when(exist)
                def _():
                    prepare(l, pieces)
        if l == layers - 1:
            sent(l)
        mixture = attend_edges(l)
        if l < layers - 1:
            ms[l, own_rows, own_cols] = (
                mixture.astype(jnp.float32)
                .reshape(tile_rows, own_blocks, HALF_COLS, inner)
                .astype(jnp.bfloat16)
            )
            sent(l)
            send(l + 1, EARLY)
            finish(l, mixture)
            send(l + 1, OUTER + DIAG)
        else:
            finish(l, mixture)


def on_device(sp_count, tp_count, grid_tokens, norm_gain, w_query, w_key, w_value, offset_bias, w_out):
    tile_rows, tile_cols, model_width = grid_tokens.shape
    layers, _, inner = w_query.shape
    tokens = tile_rows * tile_cols
    heads = inner // HEAD_DIM
    slab_rows = tile_rows + WIN_ROWS
    slab_cols = tile_cols + WIN_COLS
    slab = slab_rows * slab_cols
    flat_width = -(-(slab + tile_rows * slab_cols) // 128) * 128
    blocks = slab_cols // HALF_COLS
    bias_rows = jnp.transpose(offset_bias, (0, 2, 1, 3))
    blocked = grid_tokens.reshape(tile_rows, tile_cols // HALF_COLS, HALF_COLS, model_width)
    bf16, f32 = jnp.bfloat16, jnp.float32
    hbm = pl.BlockSpec(memory_space=pltpu.HBM)
    return pl.pallas_call(
        functools.partial(kernel, sp_count=sp_count, tp_count=tp_count),
        out_shape=jax.ShapeDtypeStruct(grid_tokens.shape, bf16),
        in_specs=[hbm] * 7,
        out_specs=pl.BlockSpec(memory_space=pltpu.VMEM),
        scratch_shapes=[
            pltpu.VMEM((slab_rows, blocks, HALF_COLS, model_width), bf16),
            pltpu.VMEM((max(layers - 1, 1), slab_rows, blocks, HALF_COLS, inner), bf16),
            pltpu.VMEM(norm_gain.shape, f32),
            pltpu.VMEM(w_query.shape, bf16),
            pltpu.VMEM(w_key.shape, bf16),
            pltpu.VMEM(w_value.shape, bf16),
            pltpu.VMEM(w_out.shape, bf16),
            pltpu.VMEM(bias_rows.shape, f32),
            pltpu.VMEM((layers * heads, flat_width), f32),
            pltpu.VMEM((tile_cols, flat_width), f32),
            pltpu.VMEM((tokens, slab), f32),
            pltpu.VMEM((layers, heads, tokens, slab), f32),
            pltpu.VMEM((slab_rows, blocks, HALF_COLS, 2 * inner), bf16),
            pltpu.VMEM((tokens, inner), bf16),
            pltpu.VMEM((tokens, model_width), f32),
            pltpu.VMEM((heads, tokens, HEAD_DIM), f32),
            pltpu.VMEM((heads, tokens, 2 * HEAD_DIM), f32),
            pltpu.SemaphoreType.DMA((3,)),
            pltpu.SemaphoreType.DMA((layers, 4)),
            pltpu.SemaphoreType.DMA((len(KINDS),)),
            pltpu.SemaphoreType.DMA((layers, len(KINDS))),
            pltpu.SemaphoreType.REGULAR((2,)),
        ],
        compiler_params=pltpu.CompilerParams(
            collective_id=0, has_side_effects=True, vmem_limit_bytes=54784 * 1024
        ),
    )(
        blocked, pltpu.with_memory_space_constraint(norm_gain, pltpu.HBM), w_query, w_key,
        w_value, pltpu.with_memory_space_constraint(bias_rows, pltpu.HBM), w_out,
    )


def solution(mesh):
    return jax.shard_map(
        functools.partial(on_device, mesh.shape["sp"], mesh.shape["tp"]),
        mesh=mesh,
        in_specs=(P(("grp", "sp"), "tp", None), P(), P(), P(), P(), P(), P()),
        out_specs=P(("grp", "sp"), "tp", None),
        check_vma=False,
    )
```

```python
import functools
import math

import jax
import jax.numpy as jnp
from jax import lax
from jax.experimental import pallas as pl
from jax.experimental.pallas import tpu as pltpu
from jax.sharding import PartitionSpec as P

HEAD_DIM = 128
WIN_ROWS = 8
WIN_COLS = 16
NORM_EPSILON = 1e-06
HALF_ROWS = WIN_ROWS // 2
HALF_COLS = WIN_COLS // 2
BELOW = WIN_ROWS - HALF_ROWS - 1
MESH = pl.DeviceIdType.MESH
LOG2E = math.log2(math.e)
HIDDEN = -1e30

KINDS = (
    "D_inner", "D_outer", "D_diag", "D_relay", "U_inner", "U_outer", "U_diag", "U_relay",
    "C_beside", "C_far",
)


def kernel(
    x_hbm, gain_hbm, wq_hbm, wk_hbm, wv_hbm, bias_hbm, wo_hbm, out,
    xs, ms, gain, wq, wk, wv, wo, bias, flat, wide, hidden, table, kv, kv_edges, queries, acc, tops, mixes,
    local_sem, w_sem, send_sem, recv_sem, entered_sem,
    *, sp_count, tp_count,
):
    layers, model_width, inner = wq.shape
    tile_rows, own_blocks = x_hbm.shape[:2]
    tile_cols = own_blocks * HALF_COLS
    tokens = tile_rows * tile_cols
    half = HALF_ROWS * tile_cols
    heads = inner // HEAD_DIM
    slab_rows = tile_rows + WIN_ROWS
    slab_cols = tile_cols + WIN_COLS
    slab = slab_rows * slab_cols
    edge = HALF_ROWS * slab_cols
    row_index = lax.axis_index("sp")
    col_index = lax.axis_index("tp")
    side = lax.rem(col_index, 2)
    beside, far = 1 - 2 * side, 2 * side - 1
    inner_block, outer_block = own_blocks - side * (own_blocks - 1), 1 + side * (own_blocks - 1)
    left_block, right_block = side * (own_blocks + 1), (1 - side) * (own_blocks + 1)

    has_above, has_below = row_index > 0, row_index < sp_count - 1
    has_beside = (col_index + beside >= 0) & (col_index + beside < tp_count)
    has_far = (col_index + far >= 0) & (col_index + far < tp_count)
    neighbours = (
        (-1, 0, has_above), (1, 0, has_below), (0, far, has_far), (0, beside, has_beside),
    )

    own_rows = slice(HALF_ROWS, HALF_ROWS + tile_rows)
    own_cols = slice(1, 1 + own_blocks)
    every_block = slice(0, own_blocks + 2)
    above_rows = slice(0, HALF_ROWS)
    last_rows = slice(tile_rows, tile_rows + HALF_ROWS)
    first_rows = slice(HALF_ROWS, HALF_ROWS + BELOW)
    below_rows = slice(HALF_ROWS + tile_rows, HALF_ROWS + tile_rows + BELOW)
    OWN = ((own_rows, own_cols),)
    BESIDE = (own_rows, pl.ds(right_block, 1))
    FAR = (own_rows, pl.ds(left_block, 1))
    ABOVE = (above_rows, every_block)
    BENEATH = (below_rows, every_block)
    EDGES = ABOVE, BENEATH

    barrier = pltpu.get_barrier_semaphore()
    for dr, dc, exists in neighbours:
        @pl.when(exists)
        def _():
            pl.semaphore_signal(
                barrier,
                inc=1,
                device_id={"sp": row_index + dr, "tp": col_index + dc},
                device_id_type=MESH,
            )

    first = [
        pltpu.make_async_copy(x_hbm, xs.at[own_rows, own_cols], local_sem.at[0]),
        pltpu.make_async_copy(gain_hbm, gain, local_sem.at[1]),
        pltpu.make_async_copy(bias_hbm, bias, local_sem.at[2]),
    ]
    for copy in first:
        copy.start()
    pairs = {"k": (wk_hbm, wk), "v": (wv_hbm, wv), "q": (wq_hbm, wq), "o": (wo_hbm, wo)}
    weight_copies = {}

    def fetch(l, names):
        for name in names:
            src, dst = pairs[name]
            copy = pltpu.make_async_copy(src.at[l], dst.at[l], w_sem.at[l, "kvqo".index(name)])
            copy.start()
            weight_copies[l, name] = copy

    def arrived(l, names):
        for name in names:
            weight_copies[l, name].wait()

    fetch(0, "kvq")

    def plan(kind):
        way, what = kind.split("_")
        if way == "C":
            if what == "beside":
                return own_rows, own_rows, inner_block, left_block, 0, beside, has_beside, has_beside
            return own_rows, own_rows, outer_block, right_block, 0, far, has_far, has_far
        dr = 1 if way == "D" else -1
        src_rows, dst_rows = (last_rows, above_rows) if dr == 1 else (first_rows, below_rows)
        goes, comes = (has_below, has_above) if dr == 1 else (has_above, has_below)
        if what == "inner":
            return src_rows, dst_rows, inner_block, inner_block, dr, 0, goes, comes
        if what == "outer":
            return src_rows, dst_rows, outer_block, outer_block, dr, 0, goes, comes
        if what == "diag":
            ends = outer_block, right_block
            return src_rows, dst_rows, *ends, dr, far, goes & has_far, comes & has_far
        passes = comes & has_beside
        return dst_rows, dst_rows, inner_block, left_block, 0, beside, passes, passes

    def halo_copy(l, kind):
        src_rows, dst_rows, src_block, dst_block, dr, dc, _, _ = plan(kind)
        ref = ms.at[l - 1] if l else xs
        i = KINDS.index(kind)
        return pltpu.make_async_remote_copy(
            src_ref=ref.at[src_rows, pl.ds(src_block, 1)],
            dst_ref=ref.at[dst_rows, pl.ds(dst_block, 1)],
            send_sem=send_sem.at[i],
            recv_sem=recv_sem.at[l, i],
            device_id={"sp": row_index + dr, "tp": col_index + dc},
            device_id_type=MESH,
        )

    def send(l, kinds):
        for kind in kinds:
            @pl.when(plan(kind)[6])
            def _():
                halo_copy(l, kind).start()

    def receive(l, kinds):
        for kind in kinds:
            @pl.when(plan(kind)[7])
            def _():
                halo_copy(l, kind).wait_recv()

    def sent(l):
        for kind in KINDS:
            @pl.when(plan(kind)[6])
            def _():
                halo_copy(l, kind).wait_send()

    def pass_on(l, way):
        receive(l, [way + "_inner"])
        send(l, [way + "_relay"])

    def shape_of(rows, cols):
        blocks = cols.size if isinstance(cols, pl.Slice) else cols.stop - cols.start
        return rows.stop - rows.start, blocks, HALF_COLS

    def zero(ref, rows, cols):
        shape = shape_of(rows, cols) + ref.shape[3:]
        ref[rows, cols] = jnp.zeros(shape, jnp.bfloat16)

    def zero_missing():
        exchanged = [xs] + [ms.at[l] for l in range(layers - 1)]
        beyond = edge + BELOW * slab_cols

        def zero_edges(low, high):
            kv_edges[low:high] = jnp.zeros((high - low, 2 * inner), jnp.bfloat16)

        zero_edges(beyond, 2 * edge)
        for exists, low, high in ((has_above, 0, edge), (has_below, edge, beyond)):
            @pl.when(jnp.logical_not(exists))
            def _():
                zero_edges(low, high)

        @pl.when(jnp.logical_not(has_far))
        def _():
            zero(kv, *FAR)

        for block in (0, own_blocks + 1):
            @pl.when(col_index == (0 if block == 0 else tp_count - 1))
            def _():
                for ref in exchanged:
                    zero(ref, slice(0, slab_rows - 1), slice(block, block + 1))

    def gather(ref, pieces):
        width = ref.shape[-1]
        return jnp.concatenate(
            [ref[rows, cols].astype(jnp.float32).reshape(-1, width) for rows, cols in pieces]
        )

    def norm(l, stream):
        factor = lax.rsqrt(jnp.mean(stream * stream, axis=-1, keepdims=True) + NORM_EPSILON)
        return (stream * gain[l : l + 1]).astype(jnp.bfloat16), factor

    def stream_of(l, pieces):
        stream = gather(xs, pieces)
        for done in range(l):
            mixture = gather(ms.at[done], pieces).astype(jnp.bfloat16)
            stream += jnp.dot(mixture, wo[done], preferred_element_type=jnp.float32)
            stream = stream.astype(jnp.bfloat16).astype(jnp.float32)
        return stream

    def project_kv(l, normed, pieces):
        scaled, factor = normed
        for i, w in enumerate((wk, wv)):
            made = jnp.dot(scaled, w[l], preferred_element_type=jnp.float32) * factor
            place = 0
            for rows, cols in pieces:
                shape = shape_of(rows, cols)
                count = math.prod(shape)
                values = made[place : place + count]
                column = slice(i * inner, (i + 1) * inner)
                if rows == own_rows:
                    kv[rows, cols, :, column] = values.reshape(*shape, inner).astype(jnp.bfloat16)
                else:
                    low = 0 if rows == above_rows else edge
                    kv_edges[low : low + count, column] = values.astype(jnp.bfloat16)
                place += count

    def project_q(l, normed):
        scaled, factor = normed
        made = jnp.dot(scaled, wq[l], preferred_element_type=jnp.float32)
        queries[...] = (made * (factor * (LOG2E / HEAD_DIM**0.5))).astype(jnp.bfloat16)

    def prepare_own(l):
        normed = norm(l, acc[...])
        project_kv(l, normed, OWN)
        project_q(l, normed)

    def prepare(l, pieces):
        project_kv(l, norm(l, stream_of(l, pieces)), pieces)

    def build_hidden():
        k = lax.broadcasted_iota(jnp.int32, (1, slab), 1)
        key_row = k // slab_cols
        key_col = k - key_row * slab_cols
        row0 = row_index * tile_rows
        col0 = col_index * tile_cols
        c = lax.broadcasted_iota(jnp.int32, (tile_cols, 1), 0)
        col_start = jnp.clip(col0 + c - HALF_COLS, 0, tp_count * tile_cols - WIN_COLS)
        col_start = col_start - (col0 - HALF_COLS)
        col_inside = (key_col >= col_start) & (key_col < col_start + WIN_COLS)
        for r in range(tile_rows):
            start = jnp.clip(row0 + r - HALF_ROWS, 0, sp_count * tile_rows - WIN_ROWS)
            start = start - (row0 - HALF_ROWS)
            row_inside = (key_row >= start) & (key_row < start + WIN_ROWS)
            hidden[r * tile_cols : (r + 1) * tile_cols] = jnp.where(
                col_inside & row_inside, 0.0, HIDDEN
            )

    lead = tile_rows - 1 - BELOW

    def build_flat():
        row_count, col_count = 2 * WIN_ROWS - 1, 2 * WIN_COLS - 1
        flat[...] = jnp.zeros_like(flat)
        for l in range(layers):
            for a in range(row_count):
                place = (lead + a) * slab_cols
                flat[l * heads : (l + 1) * heads, place : place + col_count] = bias[l, a] * LOG2E

    def build_table(l):
        width = flat.shape[1]
        shift = (width - (WIN_COLS - 1 - HALF_COLS)) % width

        def one_head(h, carry):
            spread = jnp.broadcast_to(flat[pl.ds(l * heads + h, 1), :], (tile_cols, width))
            turned = pltpu.roll(spread, shift, 1, stride=1, stride_axis=0)
            for r in range(HALF_ROWS):
                first_lane = (tile_rows - 1 - r) * slab_cols
                seen = turned[:, first_lane : first_lane + slab - edge]
                for low in (0, edge):
                    start = r * tile_cols + (half if low else 0)
                    rows = slice(start, start + tile_cols)
                    keys = slice(low, low + slab - edge)
                    table[l, h, rows, keys] = seen + hidden[rows, keys]
            return carry

        lax.fori_loop(0, heads, one_head, 0)

    def keys_values(rows):
        count = (rows.stop - rows.start) * slab_cols
        return kv[rows].astype(jnp.float32).reshape(count, 2 * inner).astype(jnp.bfloat16)

    def score(l, h, span, keys, lanes):
        return lax.dot_general(
            queries[span, h * HEAD_DIM : (h + 1) * HEAD_DIM], keys,
            (((1,), (1,)), ((), ())), preferred_element_type=jnp.float32,
        ) + table[l, h, span, lanes]

    def weigh(expo, values):
        ones = jnp.ones(values.shape, jnp.bfloat16)
        return jnp.dot(
            expo, jnp.concatenate([values, ones], axis=1),
            preferred_element_type=jnp.float32,
        )

    def attend_own(l):
        both = keys_values(own_rows)
        for h in range(heads):
            keys = both[:, h * HEAD_DIM : (h + 1) * HEAD_DIM]
            values = both[:, inner + h * HEAD_DIM : inner + (h + 1) * HEAD_DIM]
            scores = score(l, h, slice(0, tokens), keys, slice(edge, slab - edge))
            top = jnp.max(scores, axis=1, keepdims=True)
            tops[h] = jnp.broadcast_to(top, (tokens, HEAD_DIM))
            mixes[h] = weigh(jnp.exp2(scores - top).astype(jnp.bfloat16), values)

    def attend_edges(l):
        both = kv_edges[...]
        none = jnp.zeros((half, edge), jnp.bfloat16)
        mixture = []
        for h in range(heads):
            column = slice(h * HEAD_DIM, (h + 1) * HEAD_DIM)
            scores = lax.dot_general(
                queries[:, column], both[:, column],
                (((1,), (1,)), ((), ())), preferred_element_type=jnp.float32,
            )
            scores = jnp.concatenate([
                scores[:half, :edge] + table[l, h, :half, :edge],
                scores[half:, edge:] + table[l, h, half:, slab - edge :],
            ])
            top = jnp.maximum(tops[h], jnp.max(scores, axis=1, keepdims=True))
            scale = jnp.exp2(tops[h] - top)
            expo = jnp.exp2(scores - top).astype(jnp.bfloat16)
            expo = jnp.concatenate([
                jnp.concatenate([expo[:half], none], axis=1),
                jnp.concatenate([none, expo[half:]], axis=1),
            ])
            found = weigh(expo, both[:, inner + h * HEAD_DIM : inner + (h + 1) * HEAD_DIM])
            mix = mixes[h, :, :HEAD_DIM] * scale + found[:, :HEAD_DIM]
            total = mixes[h, :, HEAD_DIM:] * scale + found[:, HEAD_DIM:]
            mixture.append((mix / total).astype(jnp.bfloat16))
        return jnp.concatenate(mixture, axis=1)

    def finish(l, mixture):
        for low in range(0, model_width, 2 * HEAD_DIM):
            cols = slice(low, low + 2 * HEAD_DIM)
            stream = acc[:, cols] + jnp.dot(
                mixture, wo[l, :, cols], preferred_element_type=jnp.float32
            )
            stream = stream.astype(jnp.bfloat16)
            if l == layers - 1:
                out[:, :, cols] = stream.reshape(tile_rows, tile_cols, 2 * HEAD_DIM)
            else:
                acc[:, cols] = stream.astype(jnp.float32)

    zero_missing()
    first[0].wait()
    count = sum(jnp.where(exists, 1, 0).astype(jnp.int32) for _, _, exists in neighbours)
    pl.semaphore_wait(barrier, count)
    EARLY = ["C_beside", "D_inner", "U_inner", "C_far"]
    OUTER, DIAG = ["D_outer", "U_outer"], ["D_diag", "U_diag"]
    send(0, EARLY)
    for way, (dr, exists) in enumerate(((-1, has_above), (1, has_below))):
        @pl.when(exists & has_far)
        def _():
            pl.semaphore_signal(
                entered_sem.at[way],
                inc=1,
                device_id={"sp": row_index + dr, "tp": col_index},
                device_id_type=MESH,
            )
    fetch(0, "o")
    for later in range(1, layers):
        fetch(later, "kvqo")
    first[1].wait()
    acc[...] = gather(xs, OWN)
    for l in range(layers):
        if l == 0:
            arrived(0, "kvq")
            send(0, OUTER)
        prepare_own(l)
        if l == 0:
            for way, exists in enumerate((has_below, has_above)):
                @pl.when(exists & has_far)
                def _():
                    pl.semaphore_wait(entered_sem.at[way], 1)

            send(0, DIAG)
            build_hidden()
            first[2].wait()
            build_flat()
        build_table(l)
        if l == 0:
            arrived(0, "o")
            for later in range(1, layers):
                arrived(later, "kvqo")
        receive(l, ["C_beside"])
        prepare(l, (BESIDE,))

        @pl.when(jnp.logical_not(has_far))
        def _():
            attend_own(l)

        pass_on(l, "D")
        pass_on(l, "U")
        receive(l, ["C_far"])

        @pl.when(has_far)
        def _():
            prepare(l, (FAR,))
            attend_own(l)

        arrivals = {
            way: [way + "_" + what for what in ("outer", "diag", "relay")] for way in "UD"
        }
        receive(l, arrivals["U"] + arrivals["D"])
        for exist, pieces in (
            (has_above & has_below, EDGES),
            (has_above & jnp.logical_not(has_below), EDGES[:1]),
            (jnp.logical_not(has_above) & has_below, EDGES[1:]),
        ):
            @pl.when(exist)
            def _():
                prepare(l, pieces)
        if l == layers - 1:
            sent(l)
        mixture = attend_edges(l)
        if l < layers - 1:
            ms[l, own_rows, own_cols] = (
                mixture.astype(jnp.float32)
                .reshape(tile_rows, own_blocks, HALF_COLS, inner)
                .astype(jnp.bfloat16)
            )
            sent(l)
            send(l + 1, EARLY)
            finish(l, mixture)
            send(l + 1, OUTER + DIAG)
        else:
            finish(l, mixture)


def on_device(sp_count, tp_count, grid_tokens, norm_gain, w_query, w_key, w_value, offset_bias, w_out):
    tile_rows, tile_cols, model_width = grid_tokens.shape
    layers, _, inner = w_query.shape
    tokens = tile_rows * tile_cols
    heads = inner // HEAD_DIM
    slab_rows = tile_rows + WIN_ROWS
    slab_cols = tile_cols + WIN_COLS
    slab = slab_rows * slab_cols
    flat_width = -(-(slab + tile_rows * slab_cols) // 128) * 128
    blocks = slab_cols // HALF_COLS
    bias_rows = jnp.transpose(offset_bias, (0, 2, 1, 3))
    blocked = grid_tokens.reshape(tile_rows, tile_cols // HALF_COLS, HALF_COLS, model_width)
    bf16, f32 = jnp.bfloat16, jnp.float32
    hbm = pl.BlockSpec(memory_space=pltpu.HBM)
    return pl.pallas_call(
        functools.partial(kernel, sp_count=sp_count, tp_count=tp_count),
        out_shape=jax.ShapeDtypeStruct(grid_tokens.shape, bf16),
        in_specs=[hbm] * 7,
        out_specs=pl.BlockSpec(memory_space=pltpu.VMEM),
        scratch_shapes=[
            pltpu.VMEM((slab_rows, blocks, HALF_COLS, model_width), bf16),
            pltpu.VMEM((max(layers - 1, 1), slab_rows, blocks, HALF_COLS, inner), bf16),
            pltpu.VMEM(norm_gain.shape, f32),
            pltpu.VMEM(w_query.shape, bf16),
            pltpu.VMEM(w_key.shape, bf16),
            pltpu.VMEM(w_value.shape, bf16),
            pltpu.VMEM(w_out.shape, bf16),
            pltpu.VMEM(bias_rows.shape, f32),
            pltpu.VMEM((layers * heads, flat_width), f32),
            pltpu.VMEM((tile_cols, flat_width), f32),
            pltpu.VMEM((tokens, slab), f32),
            pltpu.VMEM((layers, heads, tokens, slab), f32),
            pltpu.VMEM((slab_rows, blocks, HALF_COLS, 2 * inner), bf16),
            pltpu.VMEM((WIN_ROWS * slab_cols, 2 * inner), bf16),
            pltpu.VMEM((tokens, inner), bf16),
            pltpu.VMEM((tokens, model_width), f32),
            pltpu.VMEM((heads, tokens, HEAD_DIM), f32),
            pltpu.VMEM((heads, tokens, 2 * HEAD_DIM), f32),
            pltpu.SemaphoreType.DMA((3,)),
            pltpu.SemaphoreType.DMA((layers, 4)),
            pltpu.SemaphoreType.DMA((len(KINDS),)),
            pltpu.SemaphoreType.DMA((layers, len(KINDS))),
            pltpu.SemaphoreType.REGULAR((2,)),
        ],
        compiler_params=pltpu.CompilerParams(
            collective_id=0, has_side_effects=True, vmem_limit_bytes=54784 * 1024
        ),
    )(
        blocked, pltpu.with_memory_space_constraint(norm_gain, pltpu.HBM), w_query, w_key,
        w_value, pltpu.with_memory_space_constraint(bias_rows, pltpu.HBM), w_out,
    )


def solution(mesh):
    return jax.shard_map(
        functools.partial(on_device, mesh.shape["sp"], mesh.shape["tp"]),
        mesh=mesh,
        in_specs=(P(("grp", "sp"), "tp", None), P(), P(), P(), P(), P(), P()),
        out_specs=P(("grp", "sp"), "tp", None),
        check_vma=False,
    )
```

```python
import functools
import math

import jax
import jax.numpy as jnp
from jax import lax
from jax.experimental import pallas as pl
from jax.experimental.pallas import tpu as pltpu
from jax.sharding import PartitionSpec as P

HEAD_DIM = 128
WIN_ROWS = 8
WIN_COLS = 16
NORM_EPSILON = 1e-06
HALF_ROWS = WIN_ROWS // 2
HALF_COLS = WIN_COLS // 2
BELOW = WIN_ROWS - HALF_ROWS - 1
MESH = pl.DeviceIdType.MESH
LOG2E = math.log2(math.e)
HIDDEN = -1e30

KINDS = (
    "D_inner", "D_outer", "D_diag", "D_relay", "U_inner", "U_outer", "U_diag", "U_relay",
    "C_beside", "C_far",
)


def kernel(
    x_hbm, gain_hbm, wq_hbm, wk_hbm, wv_hbm, bias_hbm, wo_hbm, out,
    xs, ms, gain, wq, wk, wv, wo, bias, flat, wide, hidden, table, kv, queries, acc, tops, mixes,
    local_sem, w_sem, send_sem, recv_sem, entered_sem,
    *, sp_count, tp_count,
):
    layers, model_width, inner = wq.shape
    tile_rows, own_blocks = x_hbm.shape[:2]
    tile_cols = own_blocks * HALF_COLS
    tokens = tile_rows * tile_cols
    half = HALF_ROWS * tile_cols
    heads = inner // HEAD_DIM
    slab_rows = tile_rows + WIN_ROWS
    slab_cols = tile_cols + WIN_COLS
    slab = slab_rows * slab_cols
    edge = HALF_ROWS * slab_cols
    row_index = lax.axis_index("sp")
    col_index = lax.axis_index("tp")
    side = lax.rem(col_index, 2)
    beside, far = 1 - 2 * side, 2 * side - 1
    inner_block, outer_block = own_blocks - side * (own_blocks - 1), 1 + side * (own_blocks - 1)
    left_block, right_block = side * (own_blocks + 1), (1 - side) * (own_blocks + 1)

    has_above, has_below = row_index > 0, row_index < sp_count - 1
    has_beside = (col_index + beside >= 0) & (col_index + beside < tp_count)
    has_far = (col_index + far >= 0) & (col_index + far < tp_count)
    neighbours = (
        (-1, 0, has_above), (1, 0, has_below), (0, far, has_far), (0, beside, has_beside),
    )

    own_rows = slice(HALF_ROWS, HALF_ROWS + tile_rows)
    own_cols = slice(1, 1 + own_blocks)
    every_block = slice(0, own_blocks + 2)
    above_rows = slice(0, HALF_ROWS)
    last_rows = slice(tile_rows, tile_rows + HALF_ROWS)
    first_rows = slice(HALF_ROWS, HALF_ROWS + BELOW)
    below_rows = slice(HALF_ROWS + tile_rows, HALF_ROWS + tile_rows + BELOW)
    OWN = ((own_rows, own_cols),)
    BESIDE = (own_rows, pl.ds(right_block, 1))
    FAR = (own_rows, pl.ds(left_block, 1))
    ABOVE = (above_rows, every_block)
    BENEATH = (below_rows, every_block)
    EDGES = ABOVE, BENEATH

    barrier = pltpu.get_barrier_semaphore()
    for dr, dc, exists in neighbours:
        @pl.when(exists)
        def _():
            pl.semaphore_signal(
                barrier,
                inc=1,
                device_id={"sp": row_index + dr, "tp": col_index + dc},
                device_id_type=MESH,
            )

    first = [
        pltpu.make_async_copy(x_hbm, xs.at[own_rows, own_cols], local_sem.at[0]),
        pltpu.make_async_copy(gain_hbm, gain, local_sem.at[1]),
        pltpu.make_async_copy(bias_hbm, bias, local_sem.at[2]),
    ]
    for copy in first:
        copy.start()
    pairs = {"k": (wk_hbm, wk), "v": (wv_hbm, wv), "q": (wq_hbm, wq), "o": (wo_hbm, wo)}
    weight_copies = {}

    def fetch(l, names):
        for name in names:
            src, dst = pairs[name]
            done = local_sem.at[0] if (l, name) == (0, "o") else w_sem.at[max(l - 1, 0), "kvqo".index(name)]
            copy = pltpu.make_async_copy(src.at[l], dst.at[l], done)
            copy.start()
            weight_copies[l, name] = copy

    def arrived(l, names):
        for name in names:
            weight_copies[l, name].wait()

    fetch(0, "kvq")

    def plan(kind):
        way, what = kind.split("_")
        if way == "C":
            if what == "beside":
                return own_rows, own_rows, inner_block, left_block, 0, beside, has_beside, has_beside
            return own_rows, own_rows, outer_block, right_block, 0, far, has_far, has_far
        dr = 1 if way == "D" else -1
        src_rows, dst_rows = (last_rows, above_rows) if dr == 1 else (first_rows, below_rows)
        goes, comes = (has_below, has_above) if dr == 1 else (has_above, has_below)
        if what == "inner":
            return src_rows, dst_rows, inner_block, inner_block, dr, 0, goes, comes
        if what == "outer":
            return src_rows, dst_rows, outer_block, outer_block, dr, 0, goes, comes
        if what == "diag":
            ends = outer_block, right_block
            return src_rows, dst_rows, *ends, dr, far, goes & has_far, comes & has_far
        passes = comes & has_beside
        return dst_rows, dst_rows, inner_block, left_block, 0, beside, passes, passes

    def halo_copy(l, kind):
        src_rows, dst_rows, src_block, dst_block, dr, dc, _, _ = plan(kind)
        ref = ms.at[l - 1] if l else xs
        i = KINDS.index(kind)
        return pltpu.make_async_remote_copy(
            src_ref=ref.at[src_rows, pl.ds(src_block, 1)],
            dst_ref=ref.at[dst_rows, pl.ds(dst_block, 1)],
            send_sem=send_sem.at[i],
            recv_sem=recv_sem.at[l, i],
            device_id={"sp": row_index + dr, "tp": col_index + dc},
            device_id_type=MESH,
        )

    def send(l, kinds):
        for kind in kinds:
            @pl.when(plan(kind)[6])
            def _():
                halo_copy(l, kind).start()

    def receive(l, kinds):
        for kind in kinds:
            @pl.when(plan(kind)[7])
            def _():
                halo_copy(l, kind).wait_recv()

    def sent(l):
        for kind in KINDS:
            @pl.when(plan(kind)[6])
            def _():
                halo_copy(l, kind).wait_send()

    def pass_on(l, way):
        receive(l, [way + "_inner"])
        send(l, [way + "_relay"])

    def shape_of(rows, cols):
        blocks = cols.size if isinstance(cols, pl.Slice) else cols.stop - cols.start
        return rows.stop - rows.start, blocks, HALF_COLS

    def zero(ref, rows, cols):
        shape = shape_of(rows, cols) + ref.shape[3:]
        ref[rows, cols] = jnp.zeros(shape, jnp.bfloat16)

    def zero_missing():
        exchanged = [xs] + [ms.at[l] for l in range(layers - 1)]
        zero(kv, slice(slab_rows - 1, slab_rows), every_block)
        for exists, piece in ((has_above, ABOVE), (has_below, BENEATH)):
            @pl.when(jnp.logical_not(exists))
            def _():
                zero(kv, *piece)

        @pl.when(jnp.logical_not(has_far))
        def _():
            zero(kv, *FAR)

        for block in (0, own_blocks + 1):
            @pl.when(col_index == (0 if block == 0 else tp_count - 1))
            def _():
                for ref in exchanged:
                    zero(ref, slice(0, slab_rows - 1), slice(block, block + 1))

    def gather(ref, pieces):
        width = ref.shape[-1]
        return jnp.concatenate(
            [ref[rows, cols].astype(jnp.float32).reshape(-1, width) for rows, cols in pieces]
        )

    def norm(l, stream):
        factor = lax.rsqrt(jnp.mean(stream * stream, axis=-1, keepdims=True) + NORM_EPSILON)
        return (stream * gain[l : l + 1]).astype(jnp.bfloat16), factor

    def stream_of(l, pieces):
        stream = gather(xs, pieces)
        for done in range(l):
            mixture = gather(ms.at[done], pieces).astype(jnp.bfloat16)
            stream += jnp.dot(mixture, wo[done], preferred_element_type=jnp.float32)
            stream = stream.astype(jnp.bfloat16).astype(jnp.float32)
        return stream

    def project_kv(l, normed, pieces):
        scaled, factor = normed
        for i, w in enumerate((wk, wv)):
            made = jnp.dot(scaled, w[l], preferred_element_type=jnp.float32) * factor
            place = 0
            for rows, cols in pieces:
                shape = shape_of(rows, cols)
                count = math.prod(shape)
                kv[rows, cols, :, i * inner : (i + 1) * inner] = (
                    made[place : place + count].reshape(*shape, inner).astype(jnp.bfloat16)
                )
                place += count

    def project_q(l, normed):
        scaled, factor = normed
        made = jnp.dot(scaled, wq[l], preferred_element_type=jnp.float32)
        queries[...] = (made * (factor * (LOG2E / HEAD_DIM**0.5))).astype(jnp.bfloat16)

    def prepare_own(l):
        normed = norm(l, acc[...])
        project_kv(l, normed, OWN)
        project_q(l, normed)

    def prepare(l, pieces):
        project_kv(l, norm(l, stream_of(l, pieces)), pieces)

    def build_hidden():
        k = lax.broadcasted_iota(jnp.int32, (1, slab), 1)
        key_row = k // slab_cols
        key_col = k - key_row * slab_cols
        row0 = row_index * tile_rows
        col0 = col_index * tile_cols
        c = lax.broadcasted_iota(jnp.int32, (tile_cols, 1), 0)
        col_start = jnp.clip(col0 + c - HALF_COLS, 0, tp_count * tile_cols - WIN_COLS)
        col_start = col_start - (col0 - HALF_COLS)
        col_inside = (key_col >= col_start) & (key_col < col_start + WIN_COLS)
        for r in range(tile_rows):
            start = jnp.clip(row0 + r - HALF_ROWS, 0, sp_count * tile_rows - WIN_ROWS)
            start = start - (row0 - HALF_ROWS)
            row_inside = (key_row >= start) & (key_row < start + WIN_ROWS)
            hidden[r * tile_cols : (r + 1) * tile_cols] = jnp.where(
                col_inside & row_inside, 0.0, HIDDEN
            )

    lead = tile_rows - 1 - BELOW

    def build_flat():
        row_count, col_count = 2 * WIN_ROWS - 1, 2 * WIN_COLS - 1
        flat[...] = jnp.zeros_like(flat)
        for l in range(layers):
            for a in range(row_count):
                place = (lead + a) * slab_cols
                flat[l * heads : (l + 1) * heads, place : place + col_count] = bias[l, a] * LOG2E

    def build_table(l):
        width = flat.shape[1]
        shift = (width - (WIN_COLS - 1 - HALF_COLS)) % width

        def one_head(h, carry):
            spread = jnp.broadcast_to(flat[pl.ds(l * heads + h, 1), :], (tile_cols, width))
            turned = pltpu.roll(spread, shift, 1, stride=1, stride_axis=0)
            for r in range(HALF_ROWS):
                first_lane = (tile_rows - 1 - r) * slab_cols
                seen = turned[:, first_lane : first_lane + slab - edge]
                for low in (0, edge):
                    start = r * tile_cols + (half if low else 0)
                    rows = slice(start, start + tile_cols)
                    keys = slice(low, low + slab - edge)
                    table[l, h, rows, keys] = seen + hidden[rows, keys]
            return carry

        lax.fori_loop(0, heads, one_head, 0)

    def keys_values(rows):
        count = (rows.stop - rows.start) * slab_cols
        return kv[rows].astype(jnp.float32).reshape(count, 2 * inner).astype(jnp.bfloat16)

    def score(l, h, span, keys, lanes):
        return lax.dot_general(
            queries[span, h * HEAD_DIM : (h + 1) * HEAD_DIM], keys,
            (((1,), (1,)), ((), ())), preferred_element_type=jnp.float32,
        ) + table[l, h, span, lanes]

    def weigh(expo, values):
        ones = jnp.ones(values.shape, jnp.bfloat16)
        return jnp.dot(
            expo, jnp.concatenate([values, ones], axis=1),
            preferred_element_type=jnp.float32,
        )

    def attend_own(l):
        both = keys_values(own_rows)
        for h in range(heads):
            keys = both[:, h * HEAD_DIM : (h + 1) * HEAD_DIM]
            values = both[:, inner + h * HEAD_DIM : inner + (h + 1) * HEAD_DIM]
            scores = score(l, h, slice(0, tokens), keys, slice(edge, slab - edge))
            top = jnp.max(scores, axis=1, keepdims=True)
            tops[h] = jnp.broadcast_to(top, (tokens, HEAD_DIM))
            mixes[h] = weigh(jnp.exp2(scores - top).astype(jnp.bfloat16), values)

    def attend_edges(l):
        beyond = above_rows, slice(slab_rows - HALF_ROWS, slab_rows)
        both = jnp.concatenate([keys_values(rows) for rows in beyond])
        none = jnp.zeros((half, edge), jnp.bfloat16)
        mixture = []
        for h in range(heads):
            column = slice(h * HEAD_DIM, (h + 1) * HEAD_DIM)
            scores = lax.dot_general(
                queries[:, column], both[:, column],
                (((1,), (1,)), ((), ())), preferred_element_type=jnp.float32,
            )
            scores = jnp.concatenate([
                scores[:half, :edge] + table[l, h, :half, :edge],
                scores[half:, edge:] + table[l, h, half:, slab - edge :],
            ])
            top = jnp.maximum(tops[h], jnp.max(scores, axis=1, keepdims=True))
            scale = jnp.exp2(tops[h] - top)
            expo = jnp.exp2(scores - top).astype(jnp.bfloat16)
            expo = jnp.concatenate([
                jnp.concatenate([expo[:half], none], axis=1),
                jnp.concatenate([none, expo[half:]], axis=1),
            ])
            found = weigh(expo, both[:, inner + h * HEAD_DIM : inner + (h + 1) * HEAD_DIM])
            mix = mixes[h, :, :HEAD_DIM] * scale + found[:, :HEAD_DIM]
            total = mixes[h, :, HEAD_DIM:] * scale + found[:, HEAD_DIM:]
            mixture.append((mix / total).astype(jnp.bfloat16))
        return jnp.concatenate(mixture, axis=1)

    def finish(l, mixture):
        for low in range(0, model_width, 2 * HEAD_DIM):
            cols = slice(low, low + 2 * HEAD_DIM)
            stream = acc[:, cols] + jnp.dot(
                mixture, wo[l, :, cols], preferred_element_type=jnp.float32
            )
            stream = stream.astype(jnp.bfloat16)
            if l == layers - 1:
                out[:, :, cols] = stream.reshape(tile_rows, tile_cols, 2 * HEAD_DIM)
            else:
                acc[:, cols] = stream.astype(jnp.float32)

    zero_missing()
    first[0].wait()
    count = sum(jnp.where(exists, 1, 0).astype(jnp.int32) for _, _, exists in neighbours)
    pl.semaphore_wait(barrier, count)
    EARLY = ["C_beside", "D_inner", "U_inner", "C_far"]
    OUTER, DIAG = ["D_outer", "U_outer"], ["D_diag", "U_diag"]
    send(0, EARLY)
    for way, (dr, exists) in enumerate(((-1, has_above), (1, has_below))):
        @pl.when(exists & has_far)
        def _():
            pl.semaphore_signal(
                entered_sem.at[way],
                inc=1,
                device_id={"sp": row_index + dr, "tp": col_index},
                device_id_type=MESH,
            )
    fetch(0, "o")
    first[1].wait()
    acc[...] = gather(xs, OWN)
    for l in range(layers):
        if l == 0:
            arrived(0, "kvq")
            for later in range(1, layers):
                fetch(later, "kvqo")
            send(0, OUTER)
        prepare_own(l)
        if l == 0:
            for way, exists in enumerate((has_below, has_above)):
                @pl.when(exists & has_far)
                def _():
                    pl.semaphore_wait(entered_sem.at[way], 1)

            send(0, DIAG)
            build_hidden()
            first[2].wait()
            build_flat()
        build_table(l)
        if l == 0:
            arrived(0, "o")
            for later in range(1, layers):
                arrived(later, "kvqo")
        receive(l, ["C_beside"])
        prepare(l, (BESIDE,))

        @pl.when(jnp.logical_not(has_far))
        def _():
            attend_own(l)

        pass_on(l, "U")
        pass_on(l, "D")
        receive(l, ["C_far"])

        @pl.when(has_far)
        def _():
            prepare(l, (FAR,))
            attend_own(l)

        arrivals = {
            way: [way + "_" + what for what in ("outer", "diag", "relay")] for way in "UD"
        }
        if l == 0:
            for way, exists, piece in (("D", has_above, ABOVE), ("U", has_below, BENEATH)):
                receive(l, arrivals[way])

                @pl.when(exists)
                def _():
                    prepare(l, (piece,))
        else:
            receive(l, arrivals["U"] + arrivals["D"])
            for exist, pieces in (
                (has_above & has_below, EDGES),
                (has_above & jnp.logical_not(has_below), EDGES[:1]),
                (jnp.logical_not(has_above) & has_below, EDGES[1:]),
            ):
                @pl.when(exist)
                def _():
                    prepare(l, pieces)
        if l == layers - 1:
            sent(l)
        mixture = attend_edges(l)
        if l < layers - 1:
            ms[l, own_rows, own_cols] = (
                mixture.astype(jnp.float32)
                .reshape(tile_rows, own_blocks, HALF_COLS, inner)
                .astype(jnp.bfloat16)
            )
            sent(l)
            send(l + 1, EARLY)
            finish(l, mixture)
            send(l + 1, OUTER + DIAG)
        else:
            finish(l, mixture)


def on_device(sp_count, tp_count, grid_tokens, norm_gain, w_query, w_key, w_value, offset_bias, w_out):
    tile_rows, tile_cols, model_width = grid_tokens.shape
    layers, _, inner = w_query.shape
    tokens = tile_rows * tile_cols
    heads = inner // HEAD_DIM
    slab_rows = tile_rows + WIN_ROWS
    slab_cols = tile_cols + WIN_COLS
    slab = slab_rows * slab_cols
    flat_width = -(-(slab + tile_rows * slab_cols) // 128) * 128
    blocks = slab_cols // HALF_COLS
    bias_rows = jnp.transpose(offset_bias, (0, 2, 1, 3))
    blocked = grid_tokens.reshape(tile_rows, tile_cols // HALF_COLS, HALF_COLS, model_width)
    bf16, f32 = jnp.bfloat16, jnp.float32
    hbm = pl.BlockSpec(memory_space=pltpu.HBM)
    return pl.pallas_call(
        functools.partial(kernel, sp_count=sp_count, tp_count=tp_count),
        out_shape=jax.ShapeDtypeStruct(grid_tokens.shape, bf16),
        in_specs=[hbm] * 7,
        out_specs=pl.BlockSpec(memory_space=pltpu.VMEM),
        scratch_shapes=[
            pltpu.VMEM((slab_rows, blocks, HALF_COLS, model_width), bf16),
            pltpu.VMEM((max(layers - 1, 1), slab_rows, blocks, HALF_COLS, inner), bf16),
            pltpu.VMEM(norm_gain.shape, f32),
            pltpu.VMEM(w_query.shape, bf16),
            pltpu.VMEM(w_key.shape, bf16),
            pltpu.VMEM(w_value.shape, bf16),
            pltpu.VMEM(w_out.shape, bf16),
            pltpu.VMEM(bias_rows.shape, f32),
            pltpu.VMEM((layers * heads, flat_width), f32),
            pltpu.VMEM((tile_cols, flat_width), f32),
            pltpu.VMEM((tokens, slab), f32),
            pltpu.VMEM((layers, heads, tokens, slab), f32),
            pltpu.VMEM((slab_rows, blocks, HALF_COLS, 2 * inner), bf16),
            pltpu.VMEM((tokens, inner), bf16),
            pltpu.VMEM((tokens, model_width), f32),
            pltpu.VMEM((heads, tokens, HEAD_DIM), f32),
            pltpu.VMEM((heads, tokens, 2 * HEAD_DIM), f32),
            pltpu.SemaphoreType.DMA((3,)),
            pltpu.SemaphoreType.DMA((max(layers - 1, 1), 4)),
            pltpu.SemaphoreType.DMA((len(KINDS),)),
            pltpu.SemaphoreType.DMA((layers, len(KINDS))),
            pltpu.SemaphoreType.REGULAR((2,)),
        ],
        compiler_params=pltpu.CompilerParams(
            collective_id=0, has_side_effects=True, vmem_limit_bytes=54784 * 1024
        ),
    )(
        blocked, pltpu.with_memory_space_constraint(norm_gain, pltpu.HBM), w_query, w_key,
        w_value, pltpu.with_memory_space_constraint(bias_rows, pltpu.HBM), w_out,
    )


def solution(mesh):
    return jax.shard_map(
        functools.partial(on_device, mesh.shape["sp"], mesh.shape["tp"]),
        mesh=mesh,
        in_specs=(P(("grp", "sp"), "tp", None), P(), P(), P(), P(), P(), P()),
        out_specs=P(("grp", "sp"), "tp", None),
        check_vma=False,
    )
```
